512 devices in a mesh: ep: 128 (over z, y, core), tp: 4 (over x).
Axes of the slice: x: 4, y: 8, z: 8, core: 2. Of those that a mesh axis runs over, the one named last changes fastest.
Arguments:
- tokens: bfloat16 [2048, 2048], P('ep'), may hold values from -6 to 6
- positions: int32 [2048], P('ep'), may hold values from 1024 to 16383
- state: float32 [2048, 4, 128, 128], P('ep', 'tp'), may hold values from -1 to 1
- mix_gain: float32 [2048], replicated, may hold values from 0.1 to 1.9
- w_query: bfloat16 [2048, 512], P(None, 'tp'), may hold values from -0.125 to 0.125
- w_key: bfloat16 [2048, 512], P(None, 'tp'), may hold values from -0.125 to 0.125
- w_value: bfloat16 [2048, 512], P(None, 'tp'), may hold values from -0.125 to 0.125
- w_out: bfloat16 [512, 2048], P('tp'), may hold values from -0.25 to 0.25
- ffn_gain: float32 [2048], replicated, may hold values from 0.1 to 1.9
- branch_gate: bfloat16 [2048], replicated, may hold values from -0.125 to 0.125
- dense_gate: bfloat16 [2048, 4096], P('tp', 'ep'), may hold values from -0.125 to 0.125
- dense_up: bfloat16 [2048, 4096], P('tp', 'ep'), may hold values from -0.125 to 0.125
- dense_down: bfloat16 [4096, 2048], P('ep', 'tp'), may hold values from -0.09375 to 0.09375
- routes: int32 [2048, 6], P('ep'), may hold values from 0 to 127, all different within a row; in each aligned block of 16 rows (0 to 15, 16 to 31, ...) at most 2 rows name the same one
- route_scores: float32 [2048, 6], P('ep'), may hold values from 0.05 to 1
- expert_gate: bfloat16 [128, 2048, 512], P('ep', None, 'tp'), may hold values from -0.125 to 0.125
- expert_up: bfloat16 [128, 2048, 512], P('ep', None, 'tp'), may hold values from -0.125 to 0.125
- expert_down: bfloat16 [128, 512, 2048], P('ep', 'tp'), may hold values from -0.25 to 0.25
Outputs:
- layer_out: bfloat16 [2048, 2048], P('ep', 'tp')
The draws below stay inside these ranges and needn't reach their ends.
Inputs may be any that keep to these rules, and one draw needn't show every extreme that they name: `routes`: each row names 6 different experts. In each aligned block of 16 rows (the rows of one index of ep) no expert is named by more than 2 rows, a bound that some block reaches.
All inputs are finite; a program needn't handle non-finite values.
Results may differ from the reference program's by a relative error of at most 0.012.
Values may be sent and summed in bfloat16 or wider, within the bound.
A program may use at most 64 MiB of HBM per device.

```python
import math
import jax
import jax.numpy as jnp
import numpy as np
from jax import lax

D = 2048
HEADS = 4
HEAD = 128
EXPERT_W = 512
DENSE = 4096
TOP = 6
SEQ_DEV = 16
BATCH = 2048
EXPERTS = 128
CAP = 2
N_EP = 128
N_TP = 4


def set_ends(result, stream_key, smallest, high):
    shape = result.shape
    spot = [jax.random.randint(jax.random.fold_in(stream_key, axis), (), 0, shape[axis]) for axis in range(len(shape))]
    result = result.at[tuple(spot)].set(smallest)
    longest = shape.index(max(shape))
    spot[longest] = (spot[longest] + 1) % shape[longest]
    return result.at[tuple(spot)].set(high)


def level_of(own_key, shape, split, smallest, top_value):
    gain, own = 1.0, jax.random.fold_in(own_key, 6)
    for axis_at, blocks in split:
        heights = jnp.exp(jax.random.uniform(jax.random.fold_in(own, axis_at), (blocks,), jnp.float32, smallest / len(split), top_value / len(split)))
        gain = gain * jnp.repeat(heights, shape[axis_at] // blocks).reshape([-1 if axis == axis_at else 1 for axis in range(len(shape))])
    return gain


def routed_block(stream_key, own, number, rows, count, top, reach, skew):
    sequence = jax.random.permutation(stream_key, count)
    heavy_load, ordinary = shares(count, rows * top, reach, skew, True), shares(count, rows * top, reach, skew, False)
    places = jnp.arange(count)

    def named(tallies, turn):
        used = int((tallies > 0).sum())
        fixed = max(1, used // 4)
        shifted = fixed + (places - fixed + turn * (used - fixed)) % max(1, count - fixed)
        return jnp.zeros((count,), jnp.int32).at[sequence[jnp.where(places < fixed, places, shifted)]].set(jnp.asarray(tallies, jnp.int32))

    tallies = jnp.where(number % 4 == 0, named(heavy_load, number // 4), named(ordinary, number - number // 4 - 1))
    mixed = jax.random.permutation(jax.random.fold_in(own, 3), count)
    donor, taker = mixed[0:count // 2 * 2:2], mixed[1:count // 2 * 2:2]
    room = jnp.minimum(tallies[donor] - 1, reach - tallies[taker]) // 2
    room = jnp.where((donor == sequence[0]) | (taker == sequence[0]) | (tallies[taker] == 0), 0, jnp.maximum(room, 0))
    shifted = jax.random.randint(jax.random.fold_in(own, 4), (count // 2,), 0, 1 << 20) % (room + 1)
    tallies = tallies.at[donor].add(-shifted).at[taker].add(shifted)
    labels = jnp.searchsorted(jnp.cumsum(tallies), jnp.arange(rows * top), side="right").astype(jnp.int32)
    grid = labels.reshape(top, rows).T
    grid = grid[jax.random.permutation(jax.random.fold_in(own, 1), rows)]
    turn = jax.random.randint(jax.random.fold_in(own, 2), (rows, 1), 0, top)
    return jnp.take_along_axis(grid, (jnp.arange(top)[None, :] + turn) % top, axis=1)


def shares(amount, total, reach, slope, full):
    portions = [(1 << 20) // math.isqrt(grade ** slope) + 1 for grade in range(1, amount + 1)]
    largest = reach if full else min(reach, max(-(-total // amount), total * portions[0] // sum(portions)))
    least = 1 if total - largest >= amount - 1 else 0
    holding, rest = [largest] + [least] * (amount - 1), total - largest - least * (amount - 1)
    while rest > 0:
        candidates = [i for i in range(1, amount) if holding[i] < largest] or [i for i in range(1, amount) if holding[i] < reach]
        mass, budget = sum([portions[i] for i in candidates]), rest
        for i in candidates:
            addition = min(reach - holding[i], max(1, budget * portions[i] // mass), rest)
            holding[i] = holding[i] + addition
            rest = rest - addition
    return np.array(holding)


def noise(own_key, extent, deviation, bound, cuts=(), held_as=jnp.bfloat16):
    result = jax.random.normal(own_key, extent, jnp.float32) * deviation
    if len(cuts) > 0:
        result = level_of(own_key, extent, cuts, -0.22, 0.18) * result
    return jnp.clip(result, min=-bound, max=bound).astype(held_as)


def setup_inputs(seed: int = 0) -> dict:
    arg_keys = jax.random.split(jax.random.key(seed), 19)
    tokens = noise(arg_keys[0], (BATCH, D), 1.0, 6.0, ((0, 128),))
    positions = set_ends(jax.random.randint(arg_keys[1], (BATCH,), 1024, 16384), jax.random.fold_in(arg_keys[1], 1), 1024, 16383).astype(jnp.int32)
    state = noise(arg_keys[2], (BATCH, HEADS, HEAD, HEAD), (2 * HEAD ** -0.5), 1.0, ((0, 128), (1, 4)), jnp.float32)
    mix_gain = jnp.clip(1.0 + 0.18 * jax.random.normal(arg_keys[3], (D,), jnp.float32), 0.1, 1.9)
    w_query = noise(arg_keys[4], (D, HEADS * HEAD), D ** -0.5, 0.125, ((1, 4),))
    w_key = noise(arg_keys[5], (D, HEADS * HEAD), D ** -0.5, 0.125, ((1, 4),))
    w_value = noise(arg_keys[6], (D, HEADS * HEAD), D ** -0.5, 0.125, ((1, 4),))
    w_out = noise(arg_keys[7], (HEADS * HEAD, D), (HEADS * HEAD) ** -0.5, 0.25, ((0, 4),))
    ffn_gain = jnp.clip(1.0 + 0.18 * jax.random.normal(arg_keys[8], (D,), jnp.float32), 0.1, 1.9)
    branch_gate = noise(arg_keys[9], (D,), D ** -0.5, 0.125)
    dense_gate = noise(arg_keys[10], (D, DENSE), D ** -0.5, 0.125, ((0, 4), (1, 128)))
    dense_up = noise(arg_keys[11], (D, DENSE), D ** -0.5, 0.125, ((0, 4), (1, 128)))
    dense_down = noise(arg_keys[12], (DENSE, D), DENSE ** -0.5, 0.09375, ((0, 128), (1, 4)))
    routes_keys = jax.random.split(jax.random.fold_in(arg_keys[13], 1), BATCH // SEQ_DEV)
    routes_turns = jax.random.permutation(jax.random.fold_in(arg_keys[13], 3), BATCH // SEQ_DEV)
    routes = jax.vmap(lambda own, number: routed_block(jax.random.fold_in(arg_keys[13], 2), own, number, SEQ_DEV, EXPERTS, TOP, CAP, 2))(routes_keys, routes_turns).reshape((BATCH, TOP))
    route_scores = jnp.clip(jnp.exp(math.log(1.0) - 2.9957323 * jax.random.uniform(arg_keys[14], (BATCH, TOP), jnp.float32) ** level_of(arg_keys[14], (BATCH, TOP), ((0, 128),), -0.2, 0.2)), 0.05, 1.0)
    expert_gate = noise(arg_keys[15], (EXPERTS, D, EXPERT_W), D ** -0.5, 0.125, ((0, 128), (2, 4)))
    expert_up = noise(arg_keys[16], (EXPERTS, D, EXPERT_W), D ** -0.5, 0.125, ((0, 128), (2, 4)))
    expert_down = noise(arg_keys[17], (EXPERTS, EXPERT_W, D), EXPERT_W ** -0.5, 0.25, ((0, 128), (1, 4)))
    return {"tokens": tokens, "positions": positions, "state": state, "mix_gain": mix_gain, "w_query": w_query, "w_key": w_key, "w_value": w_value, "w_out": w_out, "ffn_gain": ffn_gain, "branch_gate": branch_gate, "dense_gate": dense_gate, "dense_up": dense_up, "dense_down": dense_down, "routes": routes, "route_scores": route_scores, "expert_gate": expert_gate, "expert_up": expert_up, "expert_down": expert_down}


EPS = 1e-06

def normalize(inputs, scale_vec):
    values = inputs.astype(jnp.float32)
    return values * lax.rsqrt(lax.optimization_barrier(jnp.mean(values * values, axis=-1, keepdims=True)) + EPS) * scale_vec

def rotate(vectors, where):
    half = vectors.shape[-1] // 2
    inverse = 1.0 / 10000.0 ** jnp.linspace(0.0, 1.0, half, dtype=jnp.float32)
    angle = where.astype(jnp.float32)[:, None] * inverse[None, :]
    cosine = jnp.cos(angle)[:, None, :]
    sine = jnp.sin(angle)[:, None, :]
    first = vectors[..., :half]
    second = vectors[..., half:]
    return jnp.concatenate([first * cosine - second * sine, second * cosine + first * sine], axis=-1)

def blocked_sum(left, right, blocks):
    inner = left.shape[1] // blocks
    total = jnp.zeros((left.shape[0], right.shape[1]), jnp.float32)
    for block in range(blocks):
        partial_value = jnp.dot(left[:, block * inner:(block + 1) * inner], right[block * inner:(block + 1) * inner], preferred_element_type=jnp.float32)
        rounded = lax.optimization_barrier(partial_value.astype(jnp.bfloat16))
        total = total + rounded.astype(jnp.float32)
    return total

def reference(tokens, positions, state, mix_gain, w_query, w_key, w_value, w_out, ffn_gain, branch_gate, dense_gate, dense_up, dense_down, routes, route_scores, expert_gate, expert_up, expert_down):
    normed = normalize(tokens, mix_gain).astype(jnp.bfloat16)
    query_vec = jnp.dot(normed, w_query, preferred_element_type=jnp.float32).reshape(BATCH, HEADS, HEAD)
    key_vec = jnp.dot(normed, w_key, preferred_element_type=jnp.float32).reshape(BATCH, HEADS, HEAD)
    value_vec = jnp.dot(normed, w_value, preferred_element_type=jnp.float32).reshape(BATCH, HEADS, HEAD)
    query_vec = rotate(query_vec, positions)
    key_vec = rotate(key_vec, positions) * HEAD ** (-0.5)
    head_index = jnp.arange(HEADS, dtype=jnp.float32)
    decay_rate = 1.0 - 2.0 ** (-5.0 - 5.0 * head_index / (HEADS - 1))
    new_state = decay_rate[None, :, None, None] * state + key_vec[:, :, :, None] * value_vec[:, :, None, :]
    retrieved = jnp.einsum('bhd,bhe->bhe', query_vec, jnp.zeros_like(value_vec)) + jnp.einsum('bhd,bhde->bhe', query_vec, new_state, precision=lax.Precision.HIGHEST)
    retrieved = retrieved * lax.rsqrt(lax.optimization_barrier(jnp.mean(retrieved * retrieved, axis=-1, keepdims=True)) + EPS)
    retrieved = retrieved.reshape(BATCH, HEADS * HEAD).astype(jnp.bfloat16)
    mixer_out = blocked_sum(retrieved, w_out, N_TP)
    after_mix = tokens.astype(jnp.float32) + mixer_out
    ffn_in = normalize(after_mix, ffn_gain).astype(jnp.bfloat16)
    per_block = SEQ_DEV * TOP
    chosen = routes.reshape(N_EP, per_block)
    marks = (chosen[:, :, None] == jnp.arange(EXPERTS, dtype=jnp.int32)[None, None, :]).astype(jnp.int32)
    ranking = lax.optimization_barrier(jnp.sum((jnp.cumsum(marks, axis=1) - marks) * marks, axis=2)).astype(jnp.int32)
    source = jnp.broadcast_to(jnp.arange(N_EP, dtype=jnp.int32)[:, None], (N_EP, per_block))
    token_of = (jnp.arange(BATCH * TOP, dtype=jnp.int32) // TOP).reshape(N_EP, per_block)
    buffer = jnp.zeros((EXPERTS, N_EP, CAP, D), jnp.bfloat16).at[chosen, source, ranking].set(ffn_in[token_of])

    def one_expert(pieces):
        rows_in, gate_mat, up_mat, down_mat = pieces
        flat_rows = rows_in.reshape(N_EP * CAP, D)
        gate_pre = jnp.dot(flat_rows, gate_mat, preferred_element_type=jnp.float32)
        up_pre = jnp.dot(flat_rows, up_mat, preferred_element_type=jnp.float32)
        hidden = (jax.nn.silu(gate_pre) * up_pre).astype(jnp.bfloat16)
        return blocked_sum(hidden, down_mat, N_TP).astype(jnp.bfloat16).reshape(N_EP, CAP, D)
    results = lax.map(one_expert, (buffer, expert_gate, expert_up, expert_down))
    picked = results[chosen, source, ranking].reshape(BATCH, TOP, D).astype(jnp.float32)
    route_weights = route_scores / lax.optimization_barrier(jnp.sum(route_scores, axis=1, keepdims=True))
    experts_out = lax.optimization_barrier(jnp.sum(route_weights[:, :, None] * picked, axis=1))
    pre_gate = blocked_sum(ffn_in, dense_gate, N_TP)
    pre_up = blocked_sum(ffn_in, dense_up, N_TP)
    dense_hidden = (jax.nn.silu(pre_gate) * pre_up).astype(jnp.bfloat16)
    dense_out = jnp.dot(dense_hidden, dense_down, preferred_element_type=jnp.float32)
    branch_weight = jax.nn.sigmoid(jnp.dot(ffn_in, branch_gate, preferred_element_type=jnp.float32))
    return (after_mix + experts_out + branch_weight[:, None] * dense_out).astype(jnp.bfloat16)
```

```python
import functools

import jax
import jax.numpy as jnp
from jax import lax
from jax.experimental import pallas as pl
from jax.experimental.pallas import tpu as pltpu
from jax.sharding import PartitionSpec as P

EPS = 1e-06


MESH = pl.DeviceIdType.MESH


def trade_kernel(n, src, dst, send_sem, recv_sem):
    me = lax.axis_index("ep")
    row = lax.axis_index("tp")
    barrier = pltpu.get_barrier_semaphore()

    def greet(step, carry):
        pl.semaphore_signal(
            barrier, 1, device_id=(lax.rem(me + step, n), row), device_id_type=MESH
        )
        return carry

    lax.fori_loop(1, n, greet, 0)
    pl.semaphore_wait(barrier, n - 1)

    def send(step, carry):
        to = lax.rem(me + step, n)
        pltpu.make_async_remote_copy(
            src_ref=src.at[to],
            dst_ref=dst.at[me],
            send_sem=send_sem,
            recv_sem=recv_sem,
            device_id=(to, row),
            device_id_type=MESH,
        ).start()
        return carry

    lax.fori_loop(1, n, send, 0)
    dst[me] = src[me]
    most = pl.ds(0, n - 1)
    pltpu.make_async_copy(src.at[most], dst.at[most], send_sem).wait()
    pltpu.make_async_copy(src.at[most], dst.at[most], recv_sem).wait()


def trade(blocks, number):
    n = blocks.shape[0]
    flat = blocks.reshape(n, -1, 128)
    return pl.pallas_call(
        functools.partial(trade_kernel, n),
        name="trade",
        out_shape=jax.ShapeDtypeStruct(flat.shape, flat.dtype),
        in_specs=[pl.BlockSpec(memory_space=pltpu.VMEM)],
        out_specs=pl.BlockSpec(memory_space=pltpu.VMEM),
        scratch_shapes=[pltpu.SemaphoreType.DMA, pltpu.SemaphoreType.DMA],
        compiler_params=pltpu.CompilerParams(collective_id=number, has_side_effects=True),
    )(flat).reshape(blocks.shape)


def from_everyone(shard, axis):
    copies = jnp.broadcast_to(shard, (lax.axis_size(axis), *shard.shape))
    return lax.all_to_all(copies, axis, split_axis=0, concat_axis=0, tiled=True)


def of_everyone(shard, axis):
    return from_everyone(shard, axis).astype(jnp.float32).sum(axis=0)


def normalize(inputs, scale_vec):
    values = inputs.astype(jnp.float32)
    return values * lax.rsqrt(jnp.mean(values * values, axis=-1, keepdims=True) + EPS) * scale_vec


def rotate(vectors, where):
    half = vectors.shape[-1] // 2
    inverse = 1.0 / 10000.0 ** jnp.linspace(0.0, 1.0, half, dtype=jnp.float32)
    angle = where.astype(jnp.float32)[:, None] * inverse[None, :]
    cosine = jnp.cos(angle)[:, None, :]
    sine = jnp.sin(angle)[:, None, :]
    first = vectors[..., :half]
    second = vectors[..., half:]
    return jnp.concatenate(
        [first * cosine - second * sine, second * cosine + first * sine], axis=-1
    )


def on_device(
    tokens,
    positions,
    state,
    mix_gain,
    w_query,
    w_key,
    w_value,
    w_out,
    ffn_gain,
    branch_gate,
    dense_gate,
    dense_up,
    dense_down,
    routes,
    route_scores,
    expert_gate,
    expert_up,
    expert_down,
):
    sequences = tokens.shape[0]
    model_width = tokens.shape[1]
    tp_count = lax.axis_size("tp")
    ep_count = lax.axis_size("ep")
    columns = model_width // tp_count
    tp_index = lax.axis_index("tp")
    local_heads = state.shape[1]
    head_dim = state.shape[2]
    normed = normalize(tokens, mix_gain).astype(jnp.bfloat16)
    query_vec = jnp.dot(normed, w_query, preferred_element_type=jnp.float32).reshape(
        sequences, local_heads, head_dim
    )
    key_vec = jnp.dot(normed, w_key, preferred_element_type=jnp.float32).reshape(
        sequences, local_heads, head_dim
    )
    value_vec = jnp.dot(normed, w_value, preferred_element_type=jnp.float32).reshape(
        sequences, local_heads, head_dim
    )
    query_vec = rotate(query_vec, positions)
    key_vec = rotate(key_vec, positions) * head_dim ** (-0.5)
    all_heads = local_heads * tp_count
    head_index = (tp_index * local_heads + jnp.arange(local_heads, dtype=jnp.int32)).astype(
        jnp.float32
    )
    decay_rate = 1.0 - 2.0 ** (-5.0 - 5.0 * head_index / (all_heads - 1))
    new_state = (
        decay_rate[None, :, None, None] * state + key_vec[:, :, :, None] * value_vec[:, :, None, :]
    )
    retrieved = jnp.einsum("bhd,bhde->bhe", query_vec, new_state)
    retrieved = retrieved * lax.rsqrt(jnp.mean(retrieved * retrieved, axis=-1, keepdims=True) + EPS)
    retrieved = retrieved.reshape(sequences, local_heads * head_dim).astype(jnp.bfloat16)
    head_partial = jnp.dot(retrieved, w_out, preferred_element_type=jnp.float32).astype(
        jnp.bfloat16
    )
    mixer_out = of_everyone(head_partial.astype(jnp.float32).astype(jnp.bfloat16), "tp").astype(
        jnp.float32
    )
    after_mix = tokens.astype(jnp.float32) + mixer_out
    ffn_in = normalize(after_mix, ffn_gain).astype(jnp.bfloat16)
    own_cols = lax.dynamic_slice_in_dim(ffn_in, tp_index * columns, columns, 1)
    per_device = expert_gate.shape[0]
    experts = per_device * ep_count
    fanout = routes.shape[1]
    capacity = max(2, min(sequences, 2 * sequences * fanout // experts))
    slot_count = experts * capacity
    marks = (routes[:, :, None] == jnp.arange(experts, dtype=jnp.int32)[None, None, :]).astype(
        jnp.int32
    )
    flattened = marks.reshape(sequences * fanout, experts)
    ranking = jnp.sum((jnp.cumsum(flattened, axis=0) - flattened) * flattened, axis=1).reshape(
        sequences, fanout
    )
    slot_index = routes * capacity + ranking
    matches = jnp.arange(slot_count, dtype=jnp.int32)[:, None, None] == slot_index[None]
    placing = jnp.any(matches, axis=2).astype(jnp.bfloat16)
    route_weights = route_scores / jnp.sum(route_scores, axis=1, keepdims=True)
    combining = jnp.sum(jnp.where(matches, route_weights[None], 0.0), axis=2).T
    packed = jnp.dot(placing, ffn_in, preferred_element_type=jnp.float32).astype(jnp.bfloat16)
    packed = packed.reshape(experts, capacity, ffn_in.shape[1])
    received = trade(packed, 0)
    count = received.shape[1]
    grouped = received.reshape(ep_count, per_device, count, model_width)
    gate_pre = jnp.einsum(
        "skcd,kdw->skcw", grouped, expert_gate, preferred_element_type=jnp.float32
    )
    up_pre = jnp.einsum("skcd,kdw->skcw", grouped, expert_up, preferred_element_type=jnp.float32)
    hidden = (jax.nn.silu(gate_pre) * up_pre).astype(jnp.bfloat16)
    partial_out = jnp.einsum(
        "skcw,kwd->skcd", hidden, expert_down, preferred_element_type=jnp.float32
    )
    blocks_out = partial_out.astype(jnp.bfloat16).reshape(
        ep_count, per_device, count, tp_count, columns
    )
    traded = lax.all_to_all(blocks_out, "tp", split_axis=3, concat_axis=3, tiled=True)
    mine = jnp.sum(traded.astype(jnp.float32), axis=3).astype(jnp.bfloat16)
    mine = mine.reshape(ep_count * per_device, count, columns)
    returned = trade(mine, 1)
    experts_out = jnp.dot(combining, returned.reshape(slot_count, columns).astype(jnp.float32))
    hidden_units = dense_gate.shape[1]
    both_weights = jnp.concatenate([dense_gate, dense_up], axis=1)
    pre_parts = jnp.dot(
        lax.all_gather(own_cols, "ep", axis=0, tiled=True),
        both_weights,
        preferred_element_type=jnp.float32,
    ).astype(jnp.bfloat16)
    pre_total = of_everyone(pre_parts.astype(jnp.float32).astype(jnp.bfloat16), "tp").astype(
        jnp.float32
    )
    dense_hidden = (jax.nn.silu(pre_total[:, :hidden_units]) * pre_total[:, hidden_units:]).astype(
        jnp.bfloat16
    )
    own_hidden = lax.all_to_all(dense_hidden, "ep", split_axis=0, concat_axis=1, tiled=True)
    dense_out = jnp.dot(
        own_hidden,
        lax.all_gather(dense_down, "ep", axis=0, tiled=True),
        preferred_element_type=jnp.float32,
    )
    branch_weight = jax.nn.sigmoid(jnp.dot(ffn_in, branch_gate, preferred_element_type=jnp.float32))
    residual_cols = lax.dynamic_slice_in_dim(after_mix, tp_index * columns, columns, 1)
    layer_out = residual_cols + experts_out + branch_weight[:, None] * dense_out
    return layer_out.astype(jnp.bfloat16)


def solution(mesh):
    placed = (
        P("ep", None),
        P("ep"),
        P("ep", "tp", None, None),
        P(),
        P(None, "tp"),
        P(None, "tp"),
        P(None, "tp"),
        P("tp", None),
        P(),
        P(),
        P("tp", "ep"),
        P("tp", "ep"),
        P("ep", "tp"),
        P("ep", None),
        P("ep", None),
        P("ep", None, "tp"),
        P("ep", None, "tp"),
        P("ep", "tp", None),
    )
    return jax.shard_map(
        on_device, mesh=mesh, in_specs=placed, out_specs=P("ep", "tp"), check_vma=False
    )
```

```python
import types

import jax
import jax.numpy as jnp
import numpy as np
from jax import lax
from jax.experimental import pallas as pl
from jax.experimental.pallas import tpu as pltpu
from jax.sharding import PartitionSpec as P

EPS = 1e-06
MESH = pl.DeviceIdType.MESH
F32 = jnp.float32
BF16 = jnp.bfloat16
NZ, NY, NC, NT = 8, 8, 2, 4
ROWS = 16
WIDTH = 2048
HEAD = 128
COLS = WIDTH // NT
HID = 128
DH = 32
NE = NZ * NC
ORDER = (0, 1, 7, 2, 6, 3, 5, 4)
CHUNKS = ((0, 3), (3, 5), (5, 8))

def dot(a, b):
    return jnp.dot(a, b, preferred_element_type=F32)


def dot_nt(a, b):
    return lax.dot_general(a, b, (((1,), (1,)), ((), ())), preferred_element_type=F32)


def dot_tn(a, b):
    return lax.dot_general(a, b, (((0,), (0,)), ((), ())), preferred_element_type=F32)


def scratch_table():
    dma = pltpu.SemaphoreType.DMA
    nch = len(CHUNKS)
    return dict(
        tok=pltpu.VMEM((ROWS, WIDTH), BF16),
        pos=pltpu.VMEM((1, ROWS), jnp.int32),
        state=pltpu.VMEM((ROWS, HEAD, HEAD), F32),
        mixg=pltpu.VMEM((WIDTH // 128, 128), F32),
        wqkv=pltpu.VMEM((WIDTH, 3 * HEAD), BF16),
        wout=pltpu.VMEM((HEAD, WIDTH), BF16),
        ffng=pltpu.VMEM((WIDTH // 128, 128), F32),
        bgate=pltpu.VMEM((WIDTH // 128, 128), BF16),
        freq=pltpu.VMEM((1, 128), F32),
        ret=pltpu.VMEM((ROWS, HEAD), F32),
        hp=pltpu.VMEM((NT, ROWS, WIDTH), BF16),
        after=pltpu.VMEM((ROWS, WIDTH), F32),
        ffn=pltpu.VMEM((ROWS, WIDTH), BF16),
        x=pltpu.VMEM((NY, ROWS, COLS), BF16),
        rt=pltpu.VMEM((NY, 6, ROWS), jnp.int32),
        sc=pltpu.VMEM((NY, 6, ROWS), F32),
        bw=pltpu.VMEM((NY, ROWS, 128), F32),
        place=pltpu.VMEM((NE * ROWS, 128), BF16),
        weigh=pltpu.VMEM((NE * ROWS, 128), BF16),
        slots=pltpu.VMEM((NE, ROWS, COLS), BF16),
        got=pltpu.VMEM((NE, ROWS, COLS), BF16),
        wgu=pltpu.VMEM((NT, COLS, 2 * HID), BF16),
        wdn=pltpu.VMEM((NT, HID, COLS), BF16),
        part=pltpu.VMEM((NT, NE * ROWS, 2 * HID), BF16),
        parts=pltpu.VMEM((NT, NE * ROWS, 2 * HID), BF16),
        hid=pltpu.VMEM((NE * ROWS, HID), BF16),
        hids=pltpu.VMEM((NE * ROWS, NT * HID), BF16),
        rows=pltpu.VMEM((NE, ROWS, COLS), BF16),
        back=pltpu.VMEM((NE, ROWS, COLS), BF16),
        dg=pltpu.VMEM((NC, NZ, DH, COLS), BF16),
        du=pltpu.VMEM((NC, NZ, DH, COLS), BF16),
        dd=pltpu.VMEM((NC, NZ, DH, COLS), BF16),
        dpart=pltpu.VMEM((2, NY * ROWS, NE * DH), BF16),
        dparts=pltpu.VMEM((NT, 2, NY * ROWS // NT, NE * DH), BF16),
        dhid=pltpu.VMEM((NY * ROWS // NT, NE * DH), BF16),
        dhids=pltpu.VMEM((NY * ROWS, NE * DH), BF16),
        acc=pltpu.VMEM((NY, ROWS, COLS), BF16),
        fin=pltpu.VMEM((NY, ROWS, COLS), BF16),
        loc=dma((24,)),
        s_hp=dma,
        r_hp=dma,
        s_wgu=dma,
        r_wgu=dma,
        s_wdn=dma,
        r_wdn=dma,
        s_rt=dma,
        r_rt=dma,
        s_sc=dma,
        r_sc=dma,
        s_x=dma,
        r_x=dma,
        s_bw=dma,
        r_bw=dma,
        s_dw=dma((3,)),
        r_dw=dma((3,)),
        s_df=dma((3,)),
        r_df=dma((3,)),
        s_z=dma,
        r_z=dma((nch,)),
        s_rs=dma((nch,)),
        r_rs=dma((nch,)),
        s_ag=dma((nch,)),
        r_ag=dma((nch,)),
        s_rz=dma,
        r_rz=dma,
        s_drs=dma,
        r_drs=dma,
        s_dag=dma,
        r_dag=dma,
        s_y=dma,
        r_y=dma,
    )


def kernel(
    tokens,
    positions,
    state,
    mix_gain,
    w_query,
    w_key,
    w_value,
    w_out,
    ffn_gain,
    branch_gate,
    dense_gate,
    dense_up,
    dense_down,
    routes,
    scores,
    expert_gate,
    expert_up,
    expert_down,
    freq,
    out,
    *scratch,
):
    m = types.SimpleNamespace(**dict(zip(scratch_table(), scratch)))
    ep = lax.axis_index("ep")
    t = lax.axis_index("tp")
    z, y, c = ep // 16, (ep // 2) % 8, ep % 2

    def at(dz=0, dy=0, dc=0, dt=0):
        where = lax.rem(z + dz, NZ) * 16 + lax.rem(y + dy, NY) * 2 + lax.rem(c + dc, NC)
        return (where, lax.rem(t + dt, NT))

    def send(src, dst, s, r, dev):
        pltpu.make_async_remote_copy(
            src_ref=src, dst_ref=dst, send_sem=s, recv_sem=r, device_id=dev, device_id_type=MESH
        ).start()

    def wait(ref, sem):
        pltpu.make_async_copy(ref, ref, sem).wait()

    count = [0]

    def fetch(src, dst):
        copy = pltpu.make_async_copy(src, dst, m.loc.at[count[0]])
        count[0] += 1
        copy.start()
        return copy

    first = [
        fetch(tokens, m.tok),
        fetch(mix_gain, m.mixg),
    ]
    qkv = [
        fetch(n, m.wqkv.at[:, pl.ds(HEAD * k, HEAD)])
        for k, n in enumerate((w_query, w_key, w_value))
    ]
    turn = [fetch(positions, m.pos), fetch(freq, m.freq)]
    states = fetch(state, m.state)
    outs = fetch(w_out, m.wout)
    gains = [fetch(ffn_gain, m.ffng), fetch(branch_gate, m.bgate)]
    mine = pl.ds(pl.multiple_of(t * COLS, COLS), COLS)
    own = [
        fetch(routes, m.rt.at[0]),
        fetch(scores, m.sc.at[0]),
        fetch(expert_gate.at[mine], m.wgu.at[0, :, pl.ds(0, HID)]),
        fetch(expert_up.at[mine], m.wgu.at[0, :, pl.ds(HID, HID)]),
        fetch(expert_down.at[:, mine], m.wdn.at[0]),
        fetch(dense_gate, m.dg.at[0, 0]),
        fetch(dense_up, m.du.at[0, 0]),
        fetch(dense_down, m.dd.at[0, 0]),
    ]

    barrier = pltpu.get_barrier_semaphore()
    peers = (
        [at(dt=d) for d in range(1, NT)]
        + [at(dy=d) for d in range(1, NY)]
        + [at(dz=d, dc=e) for d in range(NZ) for e in range(NC) if d or e]
    )
    for dev in peers:
        pl.semaphore_signal(barrier, 1, device_id=dev, device_id_type=MESH)

    for copy in first:
        copy.wait()
    tok = m.tok[...].astype(F32)
    scale = lax.rsqrt(jnp.mean(tok * tok, axis=1, keepdims=True) + EPS)
    gain = m.mixg[...]
    normed = jnp.concatenate(
        [
            (tok[:, 128 * j : 128 * j + 128] * scale * gain[j : j + 1]).astype(BF16)
            for j in range(WIDTH // 128)
        ],
        axis=1,
    )
    for copy in turn:
        copy.wait()
    eye = lax.broadcasted_iota(jnp.int32, (ROWS, ROWS), 0) == lax.broadcasted_iota(
        jnp.int32, (ROWS, ROWS), 1
    )
    where = jnp.sum(
        jnp.where(eye, m.pos[...].astype(F32), 0.0), axis=1, keepdims=True
    )
    angle = where * m.freq[...]
    lane = lax.broadcasted_iota(jnp.int32, (ROWS, HEAD), 1)
    cosine = jnp.cos(angle)
    sine = jnp.where(lane < HEAD // 2, -jnp.sin(angle), jnp.sin(angle))
    for copy in qkv:
        copy.wait()
    qkv = dot(normed, m.wqkv[...])
    query, key, value = (qkv[:, HEAD * k : HEAD * (k + 1)] for k in range(3))

    def rotate(v):
        return v * cosine + pltpu.roll(v, HEAD // 2, 1) * sine

    query = rotate(query)
    key = rotate(key) * HEAD**-0.5
    head = t.astype(F32)
    decay = 1.0 - jnp.exp2(jnp.full((1, HEAD), -5.0 - 5.0 * head / (NT - 1), F32))
    columns = query.T
    states.wait()
    for s in range(ROWS):
        m.ret[pl.ds(s, 1), :] = jnp.sum(
            m.state[s] * columns[:, s : s + 1], axis=0, keepdims=True
        )
    retrieved = m.ret[...] * decay + jnp.sum(query * key, axis=1, keepdims=True) * value
    retrieved = retrieved * lax.rsqrt(
        jnp.mean(retrieved * retrieved, axis=1, keepdims=True) + EPS
    )
    outs.wait()
    m.hp[0] = dot(retrieved.astype(BF16), m.wout[...]).astype(BF16)

    pl.semaphore_wait(barrier, len(peers))

    for d in (2, 1, 3):
        send(m.hp.at[0], m.hp.at[NT - d], m.s_hp, m.r_hp, at(dt=d))
    for d in range(1, NY):
        send(routes, m.rt.at[NY - d], m.s_rt, m.r_rt, at(dy=d))
        send(scores, m.sc.at[NY - d], m.s_sc, m.r_sc, at(dy=d))
    for d in range(1, NT):
        block = pl.ds(pl.multiple_of(lax.rem(t + d, NT) * COLS, COLS), COLS)
        for k, n in enumerate((expert_gate, expert_up)):
            send(
                n.at[block],
                m.wgu.at[NT - d, :, pl.ds(HID * k, HID)],
                m.s_wgu,
                m.r_wgu,
                at(dt=d),
            )
    dense = (m.dg, m.du, m.dd)
    for k, src in enumerate((dense_gate, dense_up, dense_down)):
        for d in (4, 3, 5, 2, 6, 1, 7):
            send(src, dense[k].at[0, NZ - d], m.s_dw.at[k], m.r_dw.at[k], at(dz=d))
    for d in range(1, NT):
        block = pl.ds(pl.multiple_of(lax.rem(t + d, NT) * COLS, COLS), COLS)
        send(
            expert_down.at[:, block], m.wdn.at[NT - d], m.s_wdn, m.r_wdn, at(dt=d)
        )

    for copy in gains:
        copy.wait()
    wait(m.hp.at[pl.ds(1, NT - 1)], m.r_hp)
    after = tok
    for d in range(NT):
        after = after + m.hp[d].astype(F32)
    m.after[...] = after
    scale = lax.rsqrt(jnp.mean(after * after, axis=1, keepdims=True) + EPS)
    gain = m.ffng[...]
    gate = m.bgate[...].astype(F32)
    branch = jnp.zeros((ROWS, 128), F32)
    for j in range(WIDTH // 128):
        piece = (after[:, 128 * j : 128 * j + 128] * scale * gain[j : j + 1]).astype(BF16)
        m.ffn[:, 128 * j : 128 * j + 128] = piece
        branch = branch + piece.astype(F32) * gate[j : j + 1]
    m.x[0] = m.ffn[:, mine]
    for d in (4, 3, 5, 2, 6, 1, 7):
        send(m.x.at[0], m.x.at[NY - d], m.s_x, m.r_x, at(dy=d))
    branch = jnp.sum(branch, axis=1, keepdims=True)
    m.bw[0] = jnp.broadcast_to(1.0 / (1.0 + jnp.exp(-branch)), (ROWS, 128))
    for d in (4, 3, 5, 2, 6, 1, 7):
        send(m.bw.at[0], m.bw.at[NY - d], m.s_bw, m.r_bw, at(dy=d))

    for copy in own:
        copy.wait()
    wait(m.rt.at[pl.ds(1, NY - 1)], m.r_rt)
    wait(m.sc.at[pl.ds(1, NY - 1)], m.r_sc)
    chosen = jnp.concatenate([m.rt[d] for d in range(NY)], axis=1)
    scored = jnp.concatenate([m.sc[d] for d in range(NY)], axis=1)
    shares = scored / jnp.sum(scored, axis=0, keepdims=True)
    k = lax.broadcasted_iota(jnp.int32, (NE, 128), 0)
    lane = lax.broadcasted_iota(jnp.int32, (NE, 128), 1)
    expert = ((z + k // 2) & 7) * 16 + y * 2 + ((c + k) & 1)
    named = jnp.zeros((NE, 128), F32)
    share = jnp.zeros((NE, 128), F32)
    for n in range(6):
        hit = chosen[n : n + 1] == expert
        named = jnp.where(hit, 1.0, named)
        share = jnp.where(hit, shares[n : n + 1], share)
    a = lax.broadcasted_iota(jnp.int32, (128, 128), 0)
    b = lax.broadcasted_iota(jnp.int32, (128, 128), 1)
    ahead = jnp.where((a // ROWS == b // ROWS) & (a < b), 1.0, 0.0).astype(BF16)
    rank = dot(named.astype(BF16), ahead)
    code = jnp.where(named > 0.5, rank + (2 * (lane // ROWS)).astype(F32), -1.0)
    slot = lax.broadcasted_iota(jnp.int32, (ROWS, 128), 0).astype(F32)
    for n in range(NE):
        hit = code[n : n + 1] == slot
        m.place[pl.ds(ROWS * n, ROWS), :] = jnp.where(hit, 1.0, 0.0).astype(BF16)
        m.weigh[pl.ds(ROWS * n, ROWS), :] = jnp.where(hit, share[n : n + 1], 0.0).astype(BF16)

    wait(m.x.at[pl.ds(1, NY - 1)], m.r_x)
    x = m.x[...].reshape(NY * ROWS, COLS)
    m.slots[...] = dot(m.place[...], x).astype(BF16).reshape(NE, ROWS, COLS)
    m.got[0] = m.slots[0]

    def chunk_of(place):
        return [n for n, (lo, hi) in enumerate(CHUNKS) if lo <= place < hi][0]

    for d in ORDER:
        place = ORDER.index((NZ - d) % NZ)
        for e in range(NC):
            if d or e:
                send(
                    m.slots.at[NC * d + e],
                    m.got.at[NC * place + e],
                    m.s_z,
                    m.r_z.at[chunk_of(place)],
                    at(dz=d, dc=e),
                )

    for k, n in enumerate(dense):
        wait(n.at[0, pl.ds(1, NZ - 1)], m.r_dw.at[k])
        send(n.at[0], n.at[1], m.s_df.at[k], m.r_df.at[k], at(dc=1))
    for k, n in enumerate(dense[:2]):
        wait(n.at[1], m.r_df.at[k])
        weights = n[...].reshape(NE * DH, COLS)
        m.dpart[k] = dot_nt(x, weights).astype(BF16)
    quarter = NY * ROWS // NT
    for d in (2, 1, 3):
        block = pl.ds(pl.multiple_of(lax.rem(t + d, NT) * quarter, quarter), quarter)
        send(m.dpart.at[:, block], m.dparts.at[NT - d], m.s_drs, m.r_drs, at(dt=d))
    block = pl.ds(pl.multiple_of(t * quarter, quarter), quarter)

    wait(m.wgu.at[pl.ds(1, NT - 1)], m.r_wgu)
    spans = [(lo * NC * ROWS, (hi - lo) * NC * ROWS) for lo, hi in CHUNKS]
    for n, (lo, hi) in enumerate(CHUNKS):
        start, size = spans[n]
        begin = max(NC * lo, 1)
        wait(m.got.at[pl.ds(begin, NC * hi - begin)], m.r_z.at[n])
        rows = m.got[NC * lo : NC * hi].reshape(size, COLS)
        for d in (2, 1, 3, 0):
            m.part[d, pl.ds(start, size)] = dot(rows, m.wgu[d]).astype(BF16)
            if d:
                send(
                    m.part.at[d, pl.ds(start, size)],
                    m.parts.at[NT - d, pl.ds(start, size)],
                    m.s_rs.at[n],
                    m.r_rs.at[n],
                    at(dt=d),
                )
    for n, (start, size) in enumerate(spans):
        span = pl.ds(start, size)
        wait(m.parts.at[pl.ds(1, NT - 1), span], m.r_rs.at[n])
        total = m.part[0, span].astype(F32)
        for d in range(1, NT):
            total = total + m.parts[d, span].astype(F32)
        pre = total[:, :HID]
        hidden = (pre / (1.0 + jnp.exp(-pre)) * total[:, HID:]).astype(BF16)
        m.hid[span] = hidden
        m.hids[span, 0:HID] = hidden
        for d in (2, 1, 3):
            send(
                m.hid.at[span],
                m.hids.at[span, pl.ds(HID * (NT - d), HID)],
                m.s_ag.at[n],
                m.r_ag.at[n],
                at(dt=d),
            )
    wait(m.dparts.at[pl.ds(1, NT - 1)], m.r_drs)
    pre = m.dpart[0, block].astype(F32)
    up = m.dpart[1, block].astype(F32)
    for d in range(1, NT):
        pre = pre + m.dparts[d, 0].astype(F32)
        up = up + m.dparts[d, 1].astype(F32)
    dhidden = (pre / (1.0 + jnp.exp(-pre)) * up).astype(BF16)
    m.dhid[...] = dhidden
    m.dhids[block] = dhidden
    for d in (2, 1, 3):
        send(m.dhid, m.dhids.at[block], m.s_dag, m.r_dag, at(dt=d))
    wait(m.wdn.at[pl.ds(1, NT - 1)], m.r_wdn)
    down = m.wdn[...].reshape(NT * HID, COLS)
    for n, (start, size) in enumerate(spans):
        span = pl.ds(start, size)
        lo, hi = CHUNKS[n]
        wait(m.hids.at[span, pl.ds(HID, (NT - 1) * HID)], m.r_ag.at[n])
        m.rows[NC * lo : NC * hi] = (
            dot(m.hids[span], down).astype(BF16).reshape(NC * (hi - lo), ROWS, COLS)
        )
        for place in range(lo, hi):
            d = ORDER[place]
            for e in range(NC):
                if d or e:
                    send(
                        m.rows.at[NC * place + e],
                        m.back.at[NC * ((NZ - d) % NZ) + e],
                        m.s_rz,
                        m.r_rz,
                        at(dz=d, dc=e),
                    )
    m.back[0] = m.rows[0]
    wait(m.dd.at[1], m.r_df.at[2])
    wait(m.dhids.at[pl.ds(0, NY * ROWS - quarter)], m.r_dag)
    wait(m.bw.at[pl.ds(1, NY - 1)], m.r_bw)
    extra = dot(m.dhids[...], m.dd[...].reshape(NE * DH, COLS))
    weight = m.bw[...].reshape(NY * ROWS, 128)
    extra = jnp.concatenate(
        [extra[:, 128 * j : 128 * j + 128] * weight for j in range(COLS // 128)], axis=1
    )
    wait(m.back.at[pl.ds(1, NE - 1)], m.r_rz)
    both = extra + dot_tn(m.weigh[...], m.back[...].reshape(NE * ROWS, COLS))
    m.acc[...] = both.astype(BF16).reshape(NY, ROWS, COLS)
    for d in (4, 3, 5, 2, 6, 1, 7):
        send(m.acc.at[d], m.fin.at[NY - d], m.s_y, m.r_y, at(dy=d))
    total = m.after[:, mine] + m.acc[0].astype(F32)
    wait(m.fin.at[pl.ds(1, NY - 1)], m.r_y)
    for d in range(1, NY):
        total = total + m.fin[d].astype(F32)
    out[...] = total.astype(BF16)

    wait(m.hp.at[pl.ds(1, NT - 1)], m.s_hp)
    wait(m.rt.at[pl.ds(1, NY - 1)], m.s_rt)
    wait(m.sc.at[pl.ds(1, NY - 1)], m.s_sc)
    wait(m.wgu.at[pl.ds(1, NT - 1)], m.s_wgu)
    wait(m.wdn.at[pl.ds(1, NT - 1)], m.s_wdn)
    wait(m.x.at[pl.ds(1, NY - 1)], m.s_x)
    wait(m.bw.at[pl.ds(1, NY - 1)], m.s_bw)
    for k, n in enumerate(dense):
        wait(n.at[0, pl.ds(1, NZ - 1)], m.s_dw.at[k])
        wait(n.at[1], m.s_df.at[k])
    wait(m.got.at[pl.ds(1, NE - 1)], m.s_z)
    for n, (start, size) in enumerate(spans):
        span = pl.ds(start, size)
        wait(m.parts.at[pl.ds(1, NT - 1), span], m.s_rs.at[n])
        wait(m.hids.at[span, pl.ds(HID, (NT - 1) * HID)], m.s_ag.at[n])
    wait(m.dparts.at[pl.ds(1, NT - 1)], m.s_drs)
    wait(m.dhids.at[pl.ds(0, NY * ROWS - quarter)], m.s_dag)
    wait(m.back.at[pl.ds(1, NE - 1)], m.s_rz)
    wait(m.fin.at[pl.ds(1, NY - 1)], m.s_y)


def on_device(
    tokens,
    positions,
    state,
    mix_gain,
    w_query,
    w_key,
    w_value,
    w_out,
    ffn_gain,
    branch_gate,
    dense_gate,
    dense_up,
    dense_down,
    routes,
    route_scores,
    expert_gate,
    expert_up,
    expert_down,
):
    half = HEAD // 2
    inverse = 10000.0 ** -(np.arange(half, dtype=np.float64) / (half - 1))
    freq = jnp.asarray(np.concatenate([inverse, inverse])[None], F32)
    args = (
        tokens,
        positions.reshape(1, ROWS),
        state.reshape(ROWS, HEAD, HEAD),
        mix_gain.reshape(WIDTH // 128, 128),
        w_query,
        w_key,
        w_value,
        w_out,
        ffn_gain.reshape(WIDTH // 128, 128),
        branch_gate.reshape(WIDTH // 128, 128),
        dense_gate.T,
        dense_up.T,
        dense_down,
        routes.T,
        route_scores.T,
        expert_gate.reshape(WIDTH, HID),
        expert_up.reshape(WIDTH, HID),
        expert_down.reshape(HID, WIDTH),
        freq,
    )
    return pl.pallas_call(
        kernel,
        name="layer",
        out_shape=jax.ShapeDtypeStruct((ROWS, COLS), BF16),
        in_specs=[pl.BlockSpec(memory_space=pltpu.HBM)] * len(args),
        out_specs=pl.BlockSpec(memory_space=pltpu.VMEM),
        scratch_shapes=list(scratch_table().values()),
        compiler_params=pltpu.CompilerParams(
            collective_id=0, has_side_effects=True, vmem_limit_bytes=60 * 1024 * 1024
        ),
    )(*args)


def solution(mesh):
    placed = (
        P("ep", None),
        P("ep"),
        P("ep", "tp", None, None),
        P(),
        P(None, "tp"),
        P(None, "tp"),
        P(None, "tp"),
        P("tp", None),
        P(),
        P(),
        P("tp", "ep"),
        P("tp", "ep"),
        P("ep", "tp"),
        P("ep", None),
        P("ep", None),
        P("ep", None, "tp"),
        P("ep", None, "tp"),
        P("ep", "tp", None),
    )
    return jax.shard_map(
        on_device, mesh=mesh, in_specs=placed, out_specs=P("ep", "tp"), check_vma=False
    )
```

```python
import types

import jax
import jax.numpy as jnp
import numpy as np
from jax import lax
from jax.experimental import pallas as pl
from jax.experimental.pallas import tpu as pltpu
from jax.sharding import PartitionSpec as P

EPS = 1e-06
MESH = pl.DeviceIdType.MESH
F32 = jnp.float32
BF16 = jnp.bfloat16
NZ, NY, NC, NT = 8, 8, 2, 4
ROWS = 16
WIDTH = 2048
HEAD = 128
COLS = WIDTH // NT
HID = 128
DH = 32
NE = NZ * NC
ORDER = (4, 3, 5, 2, 6, 1, 7, 0)
CHUNKS = ((0, 3), (3, 5), (5, 8))
FAR = (4, 3, 5, 2, 6, 1, 7)

def dot(a, b):
    return jnp.dot(a, b, preferred_element_type=F32)


def dot_nt(a, b):
    return lax.dot_general(a, b, (((1,), (1,)), ((), ())), preferred_element_type=F32)


def dot_tn(a, b):
    return lax.dot_general(a, b, (((0,), (0,)), ((), ())), preferred_element_type=F32)


def scratch_table():
    dma = pltpu.SemaphoreType.DMA
    nch = len(CHUNKS)
    gathered = NY * ROWS
    return dict(
        tok=pltpu.VMEM((ROWS, WIDTH), BF16),
        pos=pltpu.VMEM((1, ROWS), jnp.int32),
        state=pltpu.VMEM((ROWS, HEAD, HEAD), F32),
        mixg=pltpu.VMEM((WIDTH // 128, 128), F32),
        wqkv=pltpu.VMEM((WIDTH, 3 * HEAD), BF16),
        wout=pltpu.VMEM((HEAD, WIDTH), BF16),
        ffng=pltpu.VMEM((WIDTH // 128, 128), F32),
        bgate=pltpu.VMEM((WIDTH // 128, 128), BF16),
        freq=pltpu.VMEM((1, 128), F32),
        ret=pltpu.VMEM((ROWS, HEAD), F32),
        hp=pltpu.VMEM((NT, ROWS, WIDTH), BF16),
        after=pltpu.VMEM((ROWS, WIDTH), F32),
        ffn=pltpu.VMEM((ROWS, WIDTH), BF16),
        x=pltpu.VMEM((NY, ROWS, 2 * COLS), BF16),
        rt=pltpu.VMEM((NY, 6, ROWS), jnp.int32),
        sc=pltpu.VMEM((NY, 6, ROWS), F32),
        place=pltpu.VMEM((NE * ROWS, 128), BF16),
        weigh=pltpu.VMEM((NE * ROWS, 128), BF16),
        slots=pltpu.VMEM((NE, ROWS, 2 * COLS), BF16),
        got=pltpu.VMEM((NE, ROWS, WIDTH), BF16),
        wgu=pltpu.VMEM((WIDTH, 2 * HID), BF16),
        wdn=pltpu.VMEM((NT, HID, COLS), BF16),
        half=pltpu.VMEM((NE * ROWS, 2 * HID), F32),
        hid=pltpu.VMEM((NE * ROWS, HID), BF16),
        hids=pltpu.VMEM((NE * ROWS, NT * HID), BF16),
        rows=pltpu.VMEM((NE, ROWS, COLS), BF16),
        back=pltpu.VMEM((NE, ROWS, COLS), BF16),
        acc=pltpu.VMEM((NY, ROWS, COLS), BF16),
        fin=pltpu.VMEM((NY, ROWS, COLS), BF16),
        dx=pltpu.VMEM((NY, ROWS, COLS), BF16),
        dg=pltpu.VMEM((NZ, DH, COLS), BF16),
        du=pltpu.VMEM((NZ, DH, COLS), BF16),
        dd=pltpu.VMEM((NZ, DH, COLS), BF16),
        dpart=pltpu.VMEM((2, 2 * gathered, NZ * DH), BF16),
        dparts=pltpu.VMEM((NT, 2, 2 * gathered // NT, NZ * DH), BF16),
        dhid=pltpu.VMEM((2 * gathered // NT, NZ * DH), BF16),
        dhids=pltpu.VMEM((2 * gathered, NZ * DH), BF16),
        dacc=pltpu.VMEM((NC * NY, ROWS, COLS), BF16),
        dfin=pltpu.VMEM((NC * NY, ROWS, COLS), BF16),
        loc=dma((32,)),
        s_hp=dma,
        r_hp=dma,
        s_wdn=dma,
        r_wdn=dma,
        s_rt=dma,
        r_rt=dma,
        s_sc=dma,
        r_sc=dma,
        s_x=dma,
        r_x=dma,
        s_dx=dma,
        r_dx=dma,
        s_dw=dma((3,)),
        r_dw=dma((3,)),
        s_z=dma,
        r_z=dma((nch,)),
        s_up=dma((nch,)),
        r_up=dma((nch,)),
        s_ag=dma((nch,)),
        r_ag=dma((nch,)),
        s_rz=dma,
        r_rz=dma,
        s_drs=dma,
        r_drs=dma,
        s_dag=dma,
        r_dag=dma,
        s_dy=dma,
        r_dy=dma,
        s_y=dma,
        r_y=dma,
    )


def kernel(
    tokens,
    positions,
    state,
    mix_gain,
    w_query,
    w_key,
    w_value,
    w_out,
    ffn_gain,
    branch_gate,
    dense_gate,
    dense_up,
    dense_down,
    routes,
    scores,
    expert_gate,
    expert_up,
    expert_down,
    freq,
    out,
    *scratch,
):
    m = types.SimpleNamespace(**dict(zip(scratch_table(), scratch)))
    ep = lax.axis_index("ep")
    t = lax.axis_index("tp")
    z, y, c = ep // 16, (ep // 2) % 8, ep % 2

    def at(a=0, b=0, dc=0, dt=0):
        to_z = lax.rem(z + a * c + b * (1 - c), NZ)
        to_y = lax.rem(y + a * (1 - c) + b * c, NY)
        return (to_z * 16 + to_y * 2 + lax.rem(c + dc, NC), lax.rem(t + dt, NT))

    def send(src, dst, s, r, dev):
        pltpu.make_async_remote_copy(
            src_ref=src, dst_ref=dst, send_sem=s, recv_sem=r, device_id=dev, device_id_type=MESH
        ).start()

    def wait(ref, sem):
        pltpu.make_async_copy(ref, ref, sem).wait()

    def block(d):
        return pl.ds(pl.multiple_of(lax.rem(t + d, NT) * COLS, COLS), COLS)

    count = [0]

    def fetch(src, dst):
        copy = pltpu.make_async_copy(src, dst, m.loc.at[count[0]])
        count[0] += 1
        copy.start()
        return copy

    first = [fetch(tokens, m.tok), fetch(mix_gain, m.mixg)]
    qkv = [
        fetch(n, m.wqkv.at[:, pl.ds(HEAD * k, HEAD)])
        for k, n in enumerate((w_query, w_key, w_value))
    ]
    turn = [fetch(positions, m.pos), fetch(freq, m.freq)]
    states = fetch(state, m.state)
    outs = fetch(w_out, m.wout)
    gains = [fetch(ffn_gain, m.ffng), fetch(branch_gate, m.bgate)]
    own = [
        fetch(routes, m.rt.at[0]),
        fetch(scores, m.sc.at[0]),
        fetch(expert_down.at[:, block(0)], m.wdn.at[0]),
        fetch(dense_gate, m.dg.at[0]),
        fetch(dense_up, m.du.at[0]),
        fetch(dense_down, m.dd.at[0]),
    ]
    experts = [
        fetch(n.at[block(d)], m.wgu.at[pl.ds(COLS * d, COLS), pl.ds(HID * k, HID)])
        for d in range(NT)
        for k, n in enumerate((expert_gate, expert_up))
    ]

    barrier = pltpu.get_barrier_semaphore()
    peers = (
        [at(dt=d) for d in range(1, NT)]
        + [at(a=d) for d in range(1, NY)]
        + [at(b=d) for d in range(1, NY)]
        + [at(a=d, dc=1) for d in range(NY)]
        + [at(b=d, dc=1) for d in range(1, NY)]
    )
    for dev in peers:
        pl.semaphore_signal(barrier, 1, device_id=dev, device_id_type=MESH)

    for copy in first:
        copy.wait()
    tok = m.tok[...].astype(F32)
    scale = lax.rsqrt(jnp.mean(tok * tok, axis=1, keepdims=True) + EPS)
    gain = m.mixg[...]
    normed = jnp.concatenate(
        [
            (tok[:, 128 * j : 128 * j + 128] * scale * gain[j : j + 1]).astype(BF16)
            for j in range(WIDTH // 128)
        ],
        axis=1,
    )
    for copy in turn:
        copy.wait()
    eye = lax.broadcasted_iota(jnp.int32, (ROWS, ROWS), 0) == lax.broadcasted_iota(
        jnp.int32, (ROWS, ROWS), 1
    )
    where = jnp.sum(jnp.where(eye, m.pos[...].astype(F32), 0.0), axis=1, keepdims=True)
    angle = where * m.freq[...]
    lane = lax.broadcasted_iota(jnp.int32, (ROWS, HEAD), 1)
    cosine = jnp.cos(angle)
    sine = jnp.where(lane < HEAD // 2, -jnp.sin(angle), jnp.sin(angle))
    for copy in qkv:
        copy.wait()
    qkv = dot(normed, m.wqkv[...])
    query, key, value = (qkv[:, HEAD * k : HEAD * (k + 1)] for k in range(3))

    def rotate(v):
        return v * cosine + pltpu.roll(v, HEAD // 2, 1) * sine

    query = rotate(query)
    key = rotate(key) * HEAD**-0.5
    head = t.astype(F32)
    decay = 1.0 - jnp.exp2(jnp.full((1, HEAD), -5.0 - 5.0 * head / (NT - 1), F32))
    columns = query.T
    states.wait()
    for s in range(ROWS):
        m.ret[pl.ds(s, 1), :] = jnp.sum(
            m.state[s] * columns[:, s : s + 1], axis=0, keepdims=True
        )
    retrieved = m.ret[...] * decay + jnp.sum(query * key, axis=1, keepdims=True) * value
    retrieved = retrieved * lax.rsqrt(
        jnp.mean(retrieved * retrieved, axis=1, keepdims=True) + EPS
    )
    outs.wait()
    m.hp[0] = dot(retrieved.astype(BF16), m.wout[...]).astype(BF16)

    pl.semaphore_wait(barrier, len(peers))

    for d in (2, 1, 3):
        send(m.hp.at[0], m.hp.at[NT - d], m.s_hp, m.r_hp, at(dt=d))
    for d in range(1, NY):
        send(routes, m.rt.at[NY - d], m.s_rt, m.r_rt, at(a=d))
        send(scores, m.sc.at[NY - d], m.s_sc, m.r_sc, at(a=d))
    dense = (m.dg, m.du, m.dd)

    def spread(k, src):
        for d in FAR:
            send(src, dense[k].at[NZ - d], m.s_dw.at[k], m.r_dw.at[k], at(b=d))

    spread(0, dense_gate)

    for copy in gains:
        copy.wait()
    wait(m.hp.at[pl.ds(1, NT - 1)], m.r_hp)
    after = tok
    for d in range(NT):
        after = after + m.hp[d].astype(F32)
    m.after[...] = after
    scale = lax.rsqrt(jnp.mean(after * after, axis=1, keepdims=True) + EPS)
    gain = m.ffng[...]
    for j in range(WIDTH // 128):
        m.ffn[:, 128 * j : 128 * j + 128] = (
            after[:, 128 * j : 128 * j + 128] * scale * gain[j : j + 1]
        ).astype(BF16)
    for d in range(2):
        m.x[0, :, COLS * d : COLS * (d + 1)] = m.ffn[:, block(d)]
    for d in FAR:
        send(m.x.at[0], m.x.at[NY - d], m.s_x, m.r_x, at(a=d))
    for d in (2, 1, 3):
        send(expert_down.at[:, block(d)], m.wdn.at[NT - d], m.s_wdn, m.r_wdn, at(dt=d))

    for copy in own:
        copy.wait()
    wait(m.rt.at[pl.ds(1, NY - 1)], m.r_rt)
    wait(m.sc.at[pl.ds(1, NY - 1)], m.r_sc)
    chosen = jnp.concatenate([m.rt[d] for d in range(NY)], axis=1)
    scored = jnp.concatenate([m.sc[d] for d in range(NY)], axis=1)
    shares = scored / jnp.sum(scored, axis=0, keepdims=True)
    k = lax.broadcasted_iota(jnp.int32, (NE, 128), 0)
    lane = lax.broadcasted_iota(jnp.int32, (NE, 128), 1)
    expert = (
        ((z + (k // 2) * (1 - c)) & 7) * 16 + ((y + (k // 2) * c) & 7) * 2 + ((c + k) & 1)
    )
    named = jnp.zeros((NE, 128), F32)
    share = jnp.zeros((NE, 128), F32)
    for n in range(6):
        hit = chosen[n : n + 1] == expert
        named = jnp.where(hit, 1.0, named)
        share = jnp.where(hit, shares[n : n + 1], share)
    a = lax.broadcasted_iota(jnp.int32, (128, 128), 0)
    b = lax.broadcasted_iota(jnp.int32, (128, 128), 1)
    ahead = jnp.where((a // ROWS == b // ROWS) & (a < b), 1.0, 0.0).astype(BF16)
    rank = dot(named.astype(BF16), ahead)
    code = jnp.where(named > 0.5, rank + (2 * (lane // ROWS)).astype(F32), -1.0)
    slot = lax.broadcasted_iota(jnp.int32, (ROWS, 128), 0).astype(F32)
    for n in range(NE):
        hit = code[n : n + 1] == slot
        m.place[pl.ds(ROWS * n, ROWS), :] = jnp.where(hit, 1.0, 0.0).astype(BF16)
        m.weigh[pl.ds(ROWS * n, ROWS), :] = jnp.where(hit, share[n : n + 1], 0.0).astype(BF16)

    left = pl.ds(0, 2 * COLS)
    wait(m.x.at[pl.ds(1, NY - 1)], m.r_x)
    m.slots[...] = (
        dot(m.place[...], m.x[...].reshape(NY * ROWS, 2 * COLS))
        .astype(BF16)
        .reshape(NE, ROWS, 2 * COLS)
    )
    m.got[NE - NC, :, left] = m.slots[0]

    def chunk_of(spot):
        return [n for n, (lo, hi) in enumerate(CHUNKS) if lo <= spot < hi][0]

    for d in FAR + (0,):
        spot = ORDER.index((NZ - d) % NZ)
        for e in range(NC):
            if d or e:
                send(
                    m.slots.at[NC * d + e],
                    m.got.at[NC * spot + e, :, left],
                    m.s_z,
                    m.r_z.at[chunk_of(spot)],
                    at(b=d, dc=e),
                )
    for d in FAR + (0,):
        send(
            m.x.at[0, :, pl.ds(0, COLS)], m.dx.at[(NY - d) % NY], m.s_dx, m.r_dx, at(b=d, dc=1)
        )

    spread(1, dense_up)

    for copy in experts:
        copy.wait()
    spans = [(lo * NC * ROWS, (hi - lo) * NC * ROWS) for lo, hi in CHUNKS]
    for n, (lo, hi) in enumerate(CHUNKS):
        start, size = spans[n]
        some = pl.ds(NC * lo, NC * (hi - lo))
        fresh = pl.ds(NC * lo, NC * (hi - lo) - (hi == NZ))
        wait(m.got.at[fresh, :, left], m.r_z.at[n])
        for k, d in ((0, 1), (1, 3)):
            send(
                m.got.at[some, :, pl.ds(COLS * k, COLS)],
                m.got.at[some, :, pl.ds(COLS * (3 - k), COLS)],
                m.s_up.at[n],
                m.r_up.at[n],
                at(dt=d),
            )
        m.half[pl.ds(start, size)] = dot(
            m.got[NC * lo : NC * hi, :, 0 : 2 * COLS].reshape(size, 2 * COLS),
            m.wgu[0 : 2 * COLS],
        )
    spread(2, dense_down)

    wait(m.dx, m.r_dx)
    gathered = NY * ROWS
    for k in range(2):
        wait(dense[k].at[pl.ds(1, NZ - 1)], m.r_dw.at[k])
        weights = dense[k][...].reshape(NZ * DH, COLS)
        m.dpart[k, 0:gathered] = dot_nt(
            m.x[:, :, 0:COLS].reshape(gathered, COLS), weights
        ).astype(BF16)
        m.dpart[k, gathered:] = dot_nt(m.dx[...].reshape(gathered, COLS), weights).astype(BF16)
    quarter = 2 * gathered // NT

    def part(d):
        return pl.ds(pl.multiple_of(lax.rem(t + d, NT) * quarter, quarter), quarter)

    for d in (2, 1, 3):
        send(m.dpart.at[:, part(d)], m.dparts.at[NT - d], m.s_drs, m.r_drs, at(dt=d))

    for n, (lo, hi) in enumerate(CHUNKS):
        start, size = spans[n]
        span = pl.ds(start, size)
        wait(m.got.at[pl.ds(NC * lo, NC * (hi - lo)), :, pl.ds(2 * COLS, 2 * COLS)], m.r_up.at[n])
        total = m.half[span] + dot(
            m.got[NC * lo : NC * hi, :, 2 * COLS :].reshape(size, 2 * COLS),
            m.wgu[2 * COLS :],
        )
        pre = total[:, :HID]
        hidden = (pre / (1.0 + jnp.exp(-pre)) * total[:, HID:]).astype(BF16)
        m.hid[span] = hidden
        m.hids[span, 0:HID] = hidden
        for d in (2, 1, 3):
            send(
                m.hid.at[span],
                m.hids.at[span, pl.ds(HID * (NT - d), HID)],
                m.s_ag.at[n],
                m.r_ag.at[n],
                at(dt=d),
            )
    wait(m.dparts.at[pl.ds(1, NT - 1)], m.r_drs)
    pre = m.dpart[0, part(0)].astype(F32)
    up = m.dpart[1, part(0)].astype(F32)
    for d in range(1, NT):
        pre = pre + m.dparts[d, 0].astype(F32)
        up = up + m.dparts[d, 1].astype(F32)
    dhidden = (pre / (1.0 + jnp.exp(-pre)) * up).astype(BF16)
    m.dhid[...] = dhidden
    m.dhids[part(0)] = dhidden
    for d in (2, 1, 3):
        send(m.dhid, m.dhids.at[part(0)], m.s_dag, m.r_dag, at(dt=d))

    wait(m.wdn.at[pl.ds(1, NT - 1)], m.r_wdn)
    down = m.wdn[...].reshape(NT * HID, COLS)
    for n, (lo, hi) in enumerate(CHUNKS):
        start, size = spans[n]
        span = pl.ds(start, size)
        wait(m.hids.at[span, pl.ds(HID, (NT - 1) * HID)], m.r_ag.at[n])
        m.rows[NC * lo : NC * hi] = (
            dot(m.hids[span], down).astype(BF16).reshape(NC * (hi - lo), ROWS, COLS)
        )
        for spot in range(lo, hi):
            d = ORDER[spot]
            for e in range(NC):
                if d or e:
                    send(
                        m.rows.at[NC * spot + e],
                        m.back.at[NC * ((NZ - d) % NZ) + e],
                        m.s_rz,
                        m.r_rz,
                        at(a=d, dc=1) if e else at(b=d),
                    )
    m.back[0] = m.rows[NE - NC]

    gate = m.bgate[...].astype(F32)
    branch = jnp.zeros((ROWS, 128), F32)
    for j in range(WIDTH // 128):
        branch = branch + m.ffn[:, 128 * j : 128 * j + 128].astype(F32) * gate[j : j + 1]
    branch = jnp.sum(branch, axis=1, keepdims=True)
    branch = 1.0 / (1.0 + jnp.exp(-branch))
    wait(dense[2].at[pl.ds(1, NZ - 1)], m.r_dw.at[2])
    wait(m.dhids.at[pl.ds(0, 2 * gathered - quarter)], m.r_dag)
    m.dacc[...] = (
        dot(m.dhids[...], m.dd[...].reshape(NZ * DH, COLS))
        .astype(BF16)
        .reshape(NC * NY, ROWS, COLS)
    )
    for d in FAR + (0,):
        for e in range(NC):
            if d or e:
                send(
                    m.dacc.at[NY * e + d],
                    m.dfin.at[NY * e + (NY - d) % NY],
                    m.s_dy,
                    m.r_dy,
                    at(a=d, dc=e),
                )

    wait(m.back.at[pl.ds(1, NE - 1)], m.r_rz)
    both = dot_tn(m.weigh[...], m.back[...].reshape(NE * ROWS, COLS))
    m.acc[...] = both.astype(BF16).reshape(NY, ROWS, COLS)
    for d in FAR:
        send(m.acc.at[d], m.fin.at[NY - d], m.s_y, m.r_y, at(a=d))
    wait(m.dfin.at[pl.ds(1, NC * NY - 1)], m.r_dy)
    total = m.dacc[0].astype(F32)
    for d in range(1, NC * NY):
        total = total + m.dfin[d].astype(F32)
    total = m.after[:, block(0)] + branch * total + m.acc[0].astype(F32)
    wait(m.fin.at[pl.ds(1, NY - 1)], m.r_y)
    for d in range(1, NY):
        total = total + m.fin[d].astype(F32)
    out[...] = total.astype(BF16)

    wait(m.hp.at[pl.ds(1, NT - 1)], m.s_hp)
    wait(m.rt.at[pl.ds(1, NY - 1)], m.s_rt)
    wait(m.sc.at[pl.ds(1, NY - 1)], m.s_sc)
    wait(m.wdn.at[pl.ds(1, NT - 1)], m.s_wdn)
    wait(m.x.at[pl.ds(1, NY - 1)], m.s_x)
    wait(m.dx, m.s_dx)
    for k in range(3):
        wait(dense[k].at[pl.ds(1, NZ - 1)], m.s_dw.at[k])
    wait(m.got.at[pl.ds(1, NE - 1), :, left], m.s_z)
    for n, (lo, hi) in enumerate(CHUNKS):
        start, size = spans[n]
        span = pl.ds(start, size)
        wait(m.got.at[pl.ds(NC * lo, NC * (hi - lo)), :, pl.ds(2 * COLS, 2 * COLS)], m.s_up.at[n])
        wait(m.hids.at[span, pl.ds(HID, (NT - 1) * HID)], m.s_ag.at[n])
    wait(m.dparts.at[pl.ds(1, NT - 1)], m.s_drs)
    wait(m.dhids.at[pl.ds(0, 2 * gathered - quarter)], m.s_dag)
    wait(m.back.at[pl.ds(1, NE - 1)], m.s_rz)
    wait(m.dfin.at[pl.ds(1, NC * NY - 1)], m.s_dy)
    wait(m.fin.at[pl.ds(1, NY - 1)], m.s_y)


def on_device(
    tokens,
    positions,
    state,
    mix_gain,
    w_query,
    w_key,
    w_value,
    w_out,
    ffn_gain,
    branch_gate,
    dense_gate,
    dense_up,
    dense_down,
    routes,
    route_scores,
    expert_gate,
    expert_up,
    expert_down,
):
    half = HEAD // 2
    inverse = 10000.0 ** -(np.arange(half, dtype=np.float64) / (half - 1))
    freq = jnp.asarray(np.concatenate([inverse, inverse])[None], F32)
    args = (
        tokens,
        positions.reshape(1, ROWS),
        state.reshape(ROWS, HEAD, HEAD),
        mix_gain.reshape(WIDTH // 128, 128),
        w_query,
        w_key,
        w_value,
        w_out,
        ffn_gain.reshape(WIDTH // 128, 128),
        branch_gate.reshape(WIDTH // 128, 128),
        dense_gate.T,
        dense_up.T,
        dense_down,
        routes.T,
        route_scores.T,
        expert_gate.reshape(WIDTH, HID),
        expert_up.reshape(WIDTH, HID),
        expert_down.reshape(HID, WIDTH),
        freq,
    )
    return pl.pallas_call(
        kernel,
        name="layer",
        out_shape=pltpu.VMEM((ROWS, COLS), BF16),
        in_specs=[pl.BlockSpec(memory_space=pltpu.HBM)] * len(args),
        out_specs=pl.BlockSpec(memory_space=pltpu.VMEM),
        scratch_shapes=list(scratch_table().values()),
        compiler_params=pltpu.CompilerParams(
            collective_id=0, has_side_effects=True, vmem_limit_bytes=60 * 1024 * 1024
        ),
    )(*args)


def solution(mesh):
    placed = (
        P("ep", None),
        P("ep"),
        P("ep", "tp", None, None),
        P(),
        P(None, "tp"),
        P(None, "tp"),
        P(None, "tp"),
        P("tp", None),
        P(),
        P(),
        P("tp", "ep"),
        P("tp", "ep"),
        P("ep", "tp"),
        P("ep", None),
        P("ep", None),
        P("ep", None, "tp"),
        P("ep", None, "tp"),
        P("ep", "tp", None),
    )
    return jax.shard_map(
        on_device, mesh=mesh, in_specs=placed, out_specs=P("ep", "tp"), check_vma=False
    )
```

```python
import types

import jax
import jax.numpy as jnp
import numpy as np
from jax import lax
from jax.experimental import pallas as pl
from jax.experimental.pallas import tpu as pltpu
from jax.sharding import PartitionSpec as P

EPS = 1e-06
MESH = pl.DeviceIdType.MESH
F32 = jnp.float32
BF16 = jnp.bfloat16
NZ, NY, NC, NT = 8, 8, 2, 4
ROWS = 16
WIDTH = 2048
HEAD = 128
COLS = WIDTH // NT
HID = 128
DH = 32
NE = NZ * NC
ORDER = (4, 3, 5, 2, 6, 1, 7, 0)
CHUNKS = ((0, 3), (3, 5), (5, 8))
FAR = (4, 3, 5, 2, 6, 1, 7)

def dot(a, b):
    return jnp.dot(a, b, preferred_element_type=F32)


def dot_nt(a, b):
    return lax.dot_general(a, b, (((1,), (1,)), ((), ())), preferred_element_type=F32)


def dot_tn(a, b):
    return lax.dot_general(a, b, (((0,), (0,)), ((), ())), preferred_element_type=F32)


def scratch_table():
    dma = pltpu.SemaphoreType.DMA
    nch = len(CHUNKS)
    gathered = NY * ROWS
    return dict(
        tok=pltpu.VMEM((ROWS, WIDTH), BF16),
        pos=pltpu.VMEM((1, ROWS), jnp.int32),
        state=pltpu.VMEM((ROWS, HEAD, HEAD), F32),
        mixg=pltpu.VMEM((WIDTH // 128, 128), F32),
        wqkv=pltpu.VMEM((WIDTH, 3 * HEAD), BF16),
        wout=pltpu.VMEM((HEAD, WIDTH), BF16),
        ffng=pltpu.VMEM((WIDTH // 128, 128), F32),
        bgate=pltpu.VMEM((WIDTH // 128, 128), BF16),
        freq=pltpu.VMEM((1, 128), F32),
        ret=pltpu.VMEM((ROWS, HEAD), F32),
        hp=pltpu.VMEM((NT, ROWS, WIDTH), BF16),
        after=pltpu.VMEM((ROWS, WIDTH), F32),
        ffn=pltpu.VMEM((ROWS, WIDTH), BF16),
        x=pltpu.VMEM((NY, ROWS, 2 * COLS), BF16),
        rt=pltpu.VMEM((NY, 6, ROWS), jnp.int32),
        sc=pltpu.VMEM((NY, 6, ROWS), F32),
        place=pltpu.VMEM((NE * ROWS, 128), BF16),
        weigh=pltpu.VMEM((NE * ROWS, 128), BF16),
        slots=pltpu.VMEM((NE, ROWS, 2 * COLS), BF16),
        got=pltpu.VMEM((NE, ROWS, WIDTH), BF16),
        wgu=pltpu.VMEM((WIDTH, 2 * HID), BF16),
        wdn=pltpu.VMEM((NT, HID, COLS), BF16),
        half=pltpu.VMEM((NE * ROWS, 2 * HID), F32),
        hid=pltpu.VMEM((NE * ROWS, HID), BF16),
        hids=pltpu.VMEM((NE * ROWS, NT * HID), BF16),
        rows=pltpu.VMEM((NE, ROWS, COLS), BF16),
        back=pltpu.VMEM((NE, ROWS, COLS), BF16),
        acc=pltpu.VMEM((NY, ROWS, COLS), BF16),
        fin=pltpu.VMEM((NY, ROWS, COLS), BF16),
        dx=pltpu.VMEM((NY, ROWS, COLS), BF16),
        dg=pltpu.VMEM((NZ, DH, COLS), BF16),
        du=pltpu.VMEM((NZ, DH, COLS), BF16),
        dd=pltpu.VMEM((NZ, DH, COLS), BF16),
        dpart=pltpu.VMEM((2, 2 * gathered, NZ * DH), BF16),
        dparts=pltpu.VMEM((NT, 2, 2 * gathered // NT, NZ * DH), BF16),
        dhid=pltpu.VMEM((2 * gathered // NT, NZ * DH), BF16),
        dhids=pltpu.VMEM((2 * gathered, NZ * DH), BF16),
        dacc=pltpu.VMEM((NC * NY, ROWS, COLS), BF16),
        dfin=pltpu.VMEM((NC * NY, ROWS, COLS), BF16),
        near=pltpu.SemaphoreType.REGULAR,
        wide=pltpu.SemaphoreType.REGULAR,
        loc=dma((32,)),
        s_hp=dma,
        r_hp=dma,
        s_wdn=dma,
        r_wdn=dma,
        s_rt=dma,
        r_rt=dma,
        s_sc=dma,
        r_sc=dma,
        s_x=dma,
        r_x=dma,
        s_dx=dma,
        r_dx=dma,
        s_dw=dma((3,)),
        r_dw=dma((3,)),
        s_z=dma,
        r_z=dma((nch,)),
        s_up=dma((nch,)),
        r_up=dma((nch,)),
        s_ag=dma((nch,)),
        r_ag=dma((nch,)),
        s_rz=dma,
        r_rz=dma,
        s_drs=dma,
        r_drs=dma,
        s_dag=dma,
        r_dag=dma,
        s_dy=dma,
        r_dy=dma,
        s_y=dma,
        r_y=dma,
    )


def kernel(
    tokens,
    positions,
    state,
    mix_gain,
    w_query,
    w_key,
    w_value,
    w_out,
    ffn_gain,
    branch_gate,
    dense_gate,
    dense_up,
    dense_down,
    routes,
    scores,
    expert_gate,
    expert_up,
    expert_down,
    freq,
    out,
    *scratch,
):
    m = types.SimpleNamespace(**dict(zip(scratch_table(), scratch)))
    ep = lax.axis_index("ep")
    t = lax.axis_index("tp")
    z, y, c = ep // 16, (ep // 2) % 8, ep % 2

    def at(a=0, b=0, dc=0, dt=0):
        to_z = lax.rem(z + a * c + b * (1 - c), NZ)
        to_y = lax.rem(y + a * (1 - c) + b * c, NY)
        return (to_z * 16 + to_y * 2 + lax.rem(c + dc, NC), lax.rem(t + dt, NT))

    def send(src, dst, s, r, dev):
        pltpu.make_async_remote_copy(
            src_ref=src, dst_ref=dst, send_sem=s, recv_sem=r, device_id=dev, device_id_type=MESH
        ).start()

    def wait(ref, sem):
        pltpu.make_async_copy(ref, ref, sem).wait()

    def block(d):
        return pl.ds(pl.multiple_of(lax.rem(t + d, NT) * COLS, COLS), COLS)

    count = [0]

    def fetch(src, dst):
        copy = pltpu.make_async_copy(src, dst, m.loc.at[count[0]])
        count[0] += 1
        copy.start()
        return copy

    first = [fetch(tokens, m.tok), fetch(mix_gain, m.mixg)]
    qkv = [
        fetch(n, m.wqkv.at[:, pl.ds(HEAD * k, HEAD)])
        for k, n in enumerate((w_query, w_key, w_value))
    ]
    turn = [fetch(positions, m.pos), fetch(freq, m.freq)]
    states = fetch(state, m.state)
    outs = fetch(w_out, m.wout)
    gains = [fetch(ffn_gain, m.ffng), fetch(branch_gate, m.bgate)]
    own = [
        fetch(routes, m.rt.at[0]),
        fetch(scores, m.sc.at[0]),
        fetch(expert_down.at[:, block(0)], m.wdn.at[0]),
        fetch(dense_gate, m.dg.at[0]),
        fetch(dense_up, m.du.at[0]),
        fetch(dense_down, m.dd.at[0]),
    ]
    experts = [
        fetch(n.at[block(d)], m.wgu.at[pl.ds(COLS * d, COLS), pl.ds(HID * k, HID)])
        for d in range(NT)
        for k, n in enumerate((expert_gate, expert_up))
    ]

    barrier = pltpu.get_barrier_semaphore()

    def greet(dz, dy, dx, core):
        to = lax.rem(z + dz, NZ) * 16 + lax.rem(y + dy, NY) * 2 + core
        pl.semaphore_signal(
            barrier, 1, device_id=(to, lax.rem(t + dx, NT)), device_id_type=MESH
        )

    for d in range(1, NT):
        greet(0, 0, d, 0)
    for d in range(1, NY):
        greet(0, d, 0, 1)
    for d in range(1, NZ):
        greet(d, 0, 0, 1)

    @pl.when(c == 0)
    def _():
        greet(0, 0, 0, 1)

    @pl.when(c == 1)
    def _():
        greet(0, 0, 0, 0)

    for copy in first:
        copy.wait()
    tok = m.tok[...].astype(F32)
    scale = lax.rsqrt(jnp.mean(tok * tok, axis=1, keepdims=True) + EPS)
    gain = m.mixg[...]
    normed = jnp.concatenate(
        [
            (tok[:, 128 * j : 128 * j + 128] * scale * gain[j : j + 1]).astype(BF16)
            for j in range(WIDTH // 128)
        ],
        axis=1,
    )
    for copy in turn:
        copy.wait()
    eye = lax.broadcasted_iota(jnp.int32, (ROWS, ROWS), 0) == lax.broadcasted_iota(
        jnp.int32, (ROWS, ROWS), 1
    )
    where = jnp.sum(jnp.where(eye, m.pos[...].astype(F32), 0.0), axis=1, keepdims=True)
    angle = where * m.freq[...]
    lane = lax.broadcasted_iota(jnp.int32, (ROWS, HEAD), 1)
    cosine = jnp.cos(angle)
    sine = jnp.where(lane < HEAD // 2, -jnp.sin(angle), jnp.sin(angle))
    for copy in qkv:
        copy.wait()
    qkv = dot(normed, m.wqkv[...])
    query, key, value = (qkv[:, HEAD * k : HEAD * (k + 1)] for k in range(3))

    def rotate(v):
        return v * cosine + pltpu.roll(v, HEAD // 2, 1) * sine

    query = rotate(query)
    key = rotate(key) * HEAD**-0.5
    head = t.astype(F32)
    decay = 1.0 - jnp.exp2(jnp.full((1, HEAD), -5.0 - 5.0 * head / (NT - 1), F32))
    columns = query.T
    states.wait()
    for s in range(ROWS):
        m.ret[pl.ds(s, 1), :] = jnp.sum(
            m.state[s] * columns[:, s : s + 1], axis=0, keepdims=True
        )
    retrieved = m.ret[...] * decay + jnp.sum(query * key, axis=1, keepdims=True) * value
    retrieved = retrieved * lax.rsqrt(
        jnp.mean(retrieved * retrieved, axis=1, keepdims=True) + EPS
    )
    outs.wait()
    m.hp[0] = dot(retrieved.astype(BF16), m.wout[...]).astype(BF16)

    gathered = NY * ROWS
    quarter = 2 * gathered // NT
    left = pl.ds(0, 2 * COLS)
    right = pl.ds(2 * COLS, 2 * COLS)
    dense = (m.dg, m.du, m.dd)

    def part(d):
        return pl.ds(pl.multiple_of(lax.rem(t + d, NT) * quarter, quarter), quarter)

    def chunk_of(spot):
        return [n for n, (lo, hi) in enumerate(CHUNKS) if lo <= spot < hi][0]

    def spread(k):
        src = (dense_gate, dense_up, dense_down)[k]
        for d in FAR:
            send(src, dense[k].at[NZ - d], m.s_dw.at[k], m.r_dw.at[k], at(b=d))

    def spread_routes():
        for d in FAR:
            send(routes, m.rt.at[NY - d], m.s_rt, m.r_rt, at(a=d))
            send(scores, m.sc.at[NY - d], m.s_sc, m.r_sc, at(a=d))

    def split_down():
        for d in (2, 1, 3):
            send(expert_down.at[:, block(d)], m.wdn.at[NT - d], m.s_wdn, m.r_wdn, at(dt=d))

    def mix():
        for d in (2, 1, 3):
            send(m.hp.at[0], m.hp.at[NT - d], m.s_hp, m.r_hp, at(dt=d))

    def gather():
        for copy in gains:
            copy.wait()
        wait(m.hp.at[pl.ds(1, NT - 1)], m.r_hp)
        after = tok
        for d in range(NT):
            after = after + m.hp[d].astype(F32)
        m.after[...] = after
        scale = lax.rsqrt(jnp.mean(after * after, axis=1, keepdims=True) + EPS)
        gain = m.ffng[...]
        for j in range(WIDTH // 128):
            m.ffn[:, 128 * j : 128 * j + 128] = (
                after[:, 128 * j : 128 * j + 128] * scale * gain[j : j + 1]
            ).astype(BF16)
        for d in range(2):
            m.x[0, :, COLS * d : COLS * (d + 1)] = m.ffn[:, block(d)]
        for d in FAR:
            send(m.x.at[0], m.x.at[NY - d], m.s_x, m.r_x, at(a=d))

    def gather_other():
        for d in FAR + (0,):
            send(
                m.x.at[0, :, pl.ds(0, COLS)],
                m.dx.at[(NY - d) % NY],
                m.s_dx,
                m.r_dx,
                at(b=d, dc=1),
            )

    def assign():
        for copy in own:
            copy.wait()
        wait(m.rt.at[pl.ds(1, NY - 1)], m.r_rt)
        wait(m.sc.at[pl.ds(1, NY - 1)], m.r_sc)
        chosen = jnp.concatenate([m.rt[d] for d in range(NY)], axis=1)
        scored = jnp.concatenate([m.sc[d] for d in range(NY)], axis=1)
        shares = scored / jnp.sum(scored, axis=0, keepdims=True)
        k = lax.broadcasted_iota(jnp.int32, (NE, 128), 0)
        lane = lax.broadcasted_iota(jnp.int32, (NE, 128), 1)
        expert = (
            ((z + (k // 2) * (1 - c)) & 7) * 16 + ((y + (k // 2) * c) & 7) * 2 + ((c + k) & 1)
        )
        named = jnp.zeros((NE, 128), F32)
        share = jnp.zeros((NE, 128), F32)
        for n in range(6):
            hit = chosen[n : n + 1] == expert
            named = jnp.where(hit, 1.0, named)
            share = jnp.where(hit, shares[n : n + 1], share)
        a = lax.broadcasted_iota(jnp.int32, (128, 128), 0)
        b = lax.broadcasted_iota(jnp.int32, (128, 128), 1)
        ahead = jnp.where((a // ROWS == b // ROWS) & (a < b), 1.0, 0.0).astype(BF16)
        rank = dot(named.astype(BF16), ahead)
        code = jnp.where(named > 0.5, rank + (2 * (lane // ROWS)).astype(F32), -1.0)
        slot = lax.broadcasted_iota(jnp.int32, (ROWS, 128), 0).astype(F32)
        for n in range(NE):
            hit = code[n : n + 1] == slot
            m.place[pl.ds(ROWS * n, ROWS), :] = jnp.where(hit, 1.0, 0.0).astype(BF16)
            m.weigh[pl.ds(ROWS * n, ROWS), :] = jnp.where(hit, share[n : n + 1], 0.0).astype(BF16)

    def dispatch():
        wait(m.x.at[pl.ds(1, NY - 1)], m.r_x)
        m.slots[...] = (
            dot(m.place[...], m.x[...].reshape(NY * ROWS, 2 * COLS))
            .astype(BF16)
            .reshape(NE, ROWS, 2 * COLS)
        )
        for spot, d in enumerate(ORDER):
            for e in range(NC):
                k = NC * ((NZ - d) % NZ) + e
                if d or e:
                    send(
                        m.slots.at[k],
                        m.got.at[NC * spot + e, :, left],
                        m.s_z,
                        m.r_z.at[chunk_of(spot)],
                        at(b=(NZ - d) % NZ, dc=e),
                    )
                else:
                    m.got[NC * spot, :, left] = m.slots[k]

    def trade(n):
        if n == 0:
            for copy in experts:
                copy.wait()
        lo, hi = CHUNKS[n]
        some = pl.ds(NC * lo, NC * (hi - lo))
        fresh = pl.ds(NC * lo, NC * (hi - lo) - (lo <= ORDER.index(0) < hi))
        wait(m.got.at[fresh, :, left], m.r_z.at[n])
        for k, d in ((0, 1), (1, 3)):
            send(
                m.got.at[some, :, pl.ds(COLS * k, COLS)],
                m.got.at[some, :, pl.ds(COLS * (3 - k), COLS)],
                m.s_up.at[n],
                m.r_up.at[n],
                at(dt=d),
            )
        size = NC * ROWS * (hi - lo)
        m.half[pl.ds(NC * ROWS * lo, size)] = dot(
            m.got[NC * lo : NC * hi, :, 0 : 2 * COLS].reshape(size, 2 * COLS),
            m.wgu[0 : 2 * COLS],
        )

    def hide(n):
        lo, hi = CHUNKS[n]
        size = NC * ROWS * (hi - lo)
        span = pl.ds(NC * ROWS * lo, size)
        wait(m.got.at[pl.ds(NC * lo, NC * (hi - lo)), :, right], m.r_up.at[n])
        total = m.half[span] + dot(
            m.got[NC * lo : NC * hi, :, 2 * COLS :].reshape(size, 2 * COLS),
            m.wgu[2 * COLS :],
        )
        pre = total[:, :HID]
        hidden = (pre / (1.0 + jnp.exp(-pre)) * total[:, HID:]).astype(BF16)
        m.hid[span] = hidden
        m.hids[span, 0:HID] = hidden
        for d in (2, 1, 3):
            send(
                m.hid.at[span],
                m.hids.at[span, pl.ds(HID * (NT - d), HID)],
                m.s_ag.at[n],
                m.r_ag.at[n],
                at(dt=d),
            )

    def answer(n):
        if n == 0:
            wait(m.wdn.at[pl.ds(1, NT - 1)], m.r_wdn)
        lo, hi = CHUNKS[n]
        size = NC * ROWS * (hi - lo)
        span = pl.ds(NC * ROWS * lo, size)
        wait(m.hids.at[span, pl.ds(HID, (NT - 1) * HID)], m.r_ag.at[n])
        m.rows[NC * lo : NC * hi] = (
            dot(m.hids[span], m.wdn[...].reshape(NT * HID, COLS))
            .astype(BF16)
            .reshape(NC * (hi - lo), ROWS, COLS)
        )
        for spot in range(lo, hi):
            d = ORDER[spot]
            for e in range(NC):
                if d or e:
                    send(
                        m.rows.at[NC * spot + e],
                        m.back.at[NC * ((NZ - d) % NZ) + e],
                        m.s_rz,
                        m.r_rz,
                        at(a=d, dc=1) if e else at(b=d),
                    )
                else:
                    m.back[0] = m.rows[NC * spot]

    def dense_in():
        wait(m.dx, m.r_dx)
        for k in range(2):
            wait(dense[k].at[pl.ds(1, NZ - 1)], m.r_dw.at[k])
            weights = dense[k][...].reshape(NZ * DH, COLS)
            m.dpart[k, 0:gathered] = dot_nt(
                m.x[:, :, 0:COLS].reshape(gathered, COLS), weights
            ).astype(BF16)
            m.dpart[k, gathered:] = dot_nt(m.dx[...].reshape(gathered, COLS), weights).astype(BF16)
        for d in (2, 1, 3):
            send(m.dpart.at[:, part(d)], m.dparts.at[NT - d], m.s_drs, m.r_drs, at(dt=d))

    def dense_hide():
        wait(m.dparts.at[pl.ds(1, NT - 1)], m.r_drs)
        pre = m.dpart[0, part(0)].astype(F32)
        up = m.dpart[1, part(0)].astype(F32)
        for d in range(1, NT):
            pre = pre + m.dparts[d, 0].astype(F32)
            up = up + m.dparts[d, 1].astype(F32)
        dhidden = (pre / (1.0 + jnp.exp(-pre)) * up).astype(BF16)
        m.dhid[...] = dhidden
        m.dhids[part(0)] = dhidden
        for d in (2, 1, 3):
            send(m.dhid, m.dhids.at[part(0)], m.s_dag, m.r_dag, at(dt=d))

    def dense_out():
        wait(dense[2].at[pl.ds(1, NZ - 1)], m.r_dw.at[2])
        wait(m.dhids.at[pl.ds(0, 2 * gathered - quarter)], m.r_dag)
        m.dacc[...] = (
            dot(m.dhids[...], m.dd[...].reshape(NZ * DH, COLS))
            .astype(BF16)
            .reshape(NC * NY, ROWS, COLS)
        )
        for d in FAR + (0,):
            for e in range(NC):
                if d or e:
                    send(
                        m.dacc.at[NY * e + d],
                        m.dfin.at[NY * e + (NY - d) % NY],
                        m.s_dy,
                        m.r_dy,
                        at(a=d, dc=e),
                    )

    def finish():
        wait(m.back.at[pl.ds(1, NE - 1)], m.r_rz)
        both = dot_tn(m.weigh[...], m.back[...].reshape(NE * ROWS, COLS))
        m.acc[...] = both.astype(BF16).reshape(NY, ROWS, COLS)
        for d in FAR:
            send(m.acc.at[d], m.fin.at[NY - d], m.s_y, m.r_y, at(a=d))
        gate = m.bgate[...].astype(F32)
        branch = jnp.zeros((ROWS, 128), F32)
        for j in range(WIDTH // 128):
            branch = branch + m.ffn[:, 128 * j : 128 * j + 128].astype(F32) * gate[j : j + 1]
        branch = jnp.sum(branch, axis=1, keepdims=True)
        branch = 1.0 / (1.0 + jnp.exp(-branch))
        wait(m.dfin.at[pl.ds(1, NC * NY - 1)], m.r_dy)
        total = m.dacc[0].astype(F32)
        for d in range(1, NC * NY):
            total = total + m.dfin[d].astype(F32)
        total = m.after[:, block(0)] + branch * total + m.acc[0].astype(F32)
        wait(m.fin.at[pl.ds(1, NY - 1)], m.r_y)
        for d in range(1, NY):
            total = total + m.fin[d].astype(F32)
        out[...] = total.astype(BF16)

    def meet(core, count, sem):
        @pl.when(c == core)
        def _():
            pl.semaphore_wait(barrier, count)
            pl.semaphore_signal(sem, 1, device_id=at(dc=1), device_id_type=MESH)

        @pl.when(c != core)
        def _():
            pl.semaphore_wait(sem, 1)

    meet(0, NC * (NT - 1) + 1, m.near)
    mix()
    meet(1, NC * (NY - 1 + NZ - 1) + 1, m.wide)
    spread_routes()
    spread(0)
    gather()
    split_down()
    assign()
    dispatch()
    gather_other()
    spread(1)
    trade(0)
    trade(1)
    trade(2)
    spread(2)
    dense_in()
    hide(0)
    hide(1)
    hide(2)
    dense_hide()
    answer(0)
    answer(1)
    answer(2)
    dense_out()
    finish()

    wait(m.hp.at[pl.ds(1, NT - 1)], m.s_hp)
    wait(m.rt.at[pl.ds(1, NY - 1)], m.s_rt)
    wait(m.sc.at[pl.ds(1, NY - 1)], m.s_sc)
    wait(m.wdn.at[pl.ds(1, NT - 1)], m.s_wdn)
    wait(m.x.at[pl.ds(1, NY - 1)], m.s_x)
    wait(m.dx, m.s_dx)
    for k in range(3):
        wait(dense[k].at[pl.ds(1, NZ - 1)], m.s_dw.at[k])
    wait(m.got.at[pl.ds(1, NE - 1), :, left], m.s_z)
    for n, (lo, hi) in enumerate(CHUNKS):
        span = pl.ds(NC * ROWS * lo, NC * ROWS * (hi - lo))
        wait(m.got.at[pl.ds(NC * lo, NC * (hi - lo)), :, right], m.s_up.at[n])
        wait(m.hids.at[span, pl.ds(HID, (NT - 1) * HID)], m.s_ag.at[n])
    wait(m.dparts.at[pl.ds(1, NT - 1)], m.s_drs)
    wait(m.dhids.at[pl.ds(0, 2 * gathered - quarter)], m.s_dag)
    wait(m.back.at[pl.ds(1, NE - 1)], m.s_rz)
    wait(m.dfin.at[pl.ds(1, NC * NY - 1)], m.s_dy)
    wait(m.fin.at[pl.ds(1, NY - 1)], m.s_y)


def on_device(
    tokens,
    positions,
    state,
    mix_gain,
    w_query,
    w_key,
    w_value,
    w_out,
    ffn_gain,
    branch_gate,
    dense_gate,
    dense_up,
    dense_down,
    routes,
    route_scores,
    expert_gate,
    expert_up,
    expert_down,
):
    half = HEAD // 2
    inverse = 10000.0 ** -(np.arange(half, dtype=np.float64) / (half - 1))
    freq = jnp.asarray(np.concatenate([inverse, inverse])[None], F32)
    args = (
        tokens,
        positions.reshape(1, ROWS),
        state.reshape(ROWS, HEAD, HEAD),
        mix_gain.reshape(WIDTH // 128, 128),
        w_query,
        w_key,
        w_value,
        w_out,
        ffn_gain.reshape(WIDTH // 128, 128),
        branch_gate.reshape(WIDTH // 128, 128),
        dense_gate.T,
        dense_up.T,
        dense_down,
        routes.T,
        route_scores.T,
        expert_gate.reshape(WIDTH, HID),
        expert_up.reshape(WIDTH, HID),
        expert_down.reshape(HID, WIDTH),
        freq,
    )
    return pl.pallas_call(
        kernel,
        name="layer",
        out_shape=pltpu.VMEM((ROWS, COLS), BF16),
        in_specs=[pl.BlockSpec(memory_space=pltpu.HBM)] * len(args),
        out_specs=pl.BlockSpec(memory_space=pltpu.VMEM),
        scratch_shapes=list(scratch_table().values()),
        compiler_params=pltpu.CompilerParams(
            collective_id=0, has_side_effects=True, vmem_limit_bytes=60 * 1024 * 1024
        ),
    )(*args)


def solution(mesh):
    placed = (
        P("ep", None),
        P("ep"),
        P("ep", "tp", None, None),
        P(),
        P(None, "tp"),
        P(None, "tp"),
        P(None, "tp"),
        P("tp", None),
        P(),
        P(),
        P("tp", "ep"),
        P("tp", "ep"),
        P("ep", "tp"),
        P("ep", None),
        P("ep", None),
        P("ep", None, "tp"),
        P("ep", None, "tp"),
        P("ep", "tp", None),
    )
    return jax.shard_map(
        on_device, mesh=mesh, in_specs=placed, out_specs=P("ep", "tp"), check_vma=False
    )
```

```python
import types

import jax
import jax.numpy as jnp
import numpy as np
from jax import lax
from jax.experimental import pallas as pl
from jax.experimental.pallas import tpu as pltpu
from jax.sharding import PartitionSpec as P

EPS = 1e-06
MESH = pl.DeviceIdType.MESH
F32 = jnp.float32
BF16 = jnp.bfloat16
NZ, NY, NC, NT = 8, 8, 2, 4
ROWS = 16
WIDTH = 2048
HEAD = 128
COLS = WIDTH // NT
HID = 128
DH = 32
NE = NZ * NC
ORDER = (0, 1, 7, 2, 6, 3, 5, 4)
CHUNKS = ((0, 3), (3, 5), (5, 7), (7, 8))
FAR = (4, 3, 5, 2, 6, 1, 7)

def dot(a, b):
    return jnp.dot(a, b, preferred_element_type=F32)


def dot_nt(a, b):
    return lax.dot_general(a, b, (((1,), (1,)), ((), ())), preferred_element_type=F32)


def dot_tn(a, b):
    return lax.dot_general(a, b, (((0,), (0,)), ((), ())), preferred_element_type=F32)


def scratch_table():
    dma = pltpu.SemaphoreType.DMA
    nch = len(CHUNKS)
    gathered = NY * ROWS
    return dict(
        tok=pltpu.VMEM((ROWS, WIDTH), BF16),
        pos=pltpu.VMEM((1, ROWS), jnp.int32),
        state=pltpu.VMEM((ROWS, HEAD, HEAD), F32),
        mixg=pltpu.VMEM((WIDTH // 128, 128), F32),
        wqkv=pltpu.VMEM((WIDTH, 3 * HEAD), BF16),
        wout=pltpu.VMEM((HEAD, WIDTH), BF16),
        ffng=pltpu.VMEM((WIDTH // 128, 128), F32),
        bgate=pltpu.VMEM((WIDTH // 128, 128), BF16),
        freq=pltpu.VMEM((1, 128), F32),
        ret=pltpu.VMEM((ROWS, HEAD), F32),
        hp=pltpu.VMEM((NT, ROWS, WIDTH), BF16),
        after=pltpu.VMEM((ROWS, WIDTH), F32),
        ffn=pltpu.VMEM((ROWS, WIDTH), BF16),
        x=pltpu.VMEM((NY, ROWS, 2 * COLS), BF16),
        rt=pltpu.VMEM((NY, 6, ROWS), jnp.int32),
        sc=pltpu.VMEM((NY, 6, ROWS), F32),
        place=pltpu.VMEM((NE * ROWS, 128), BF16),
        weigh=pltpu.VMEM((NE * ROWS, 128), BF16),
        slots=pltpu.VMEM((NE, ROWS, 2 * COLS), BF16),
        got=pltpu.VMEM((NE, ROWS, WIDTH), BF16),
        wgu=pltpu.VMEM((WIDTH, 2 * HID), BF16),
        wdn=pltpu.VMEM((NT, HID, COLS), BF16),
        half=pltpu.VMEM((NE * ROWS, 2 * HID), F32),
        hid=pltpu.VMEM((NE * ROWS, HID), BF16),
        hids=pltpu.VMEM((NE * ROWS, NT * HID), BF16),
        rows=pltpu.VMEM((NE, ROWS, COLS), BF16),
        back=pltpu.VMEM((NE, ROWS, COLS), BF16),
        acc=pltpu.VMEM((NY, ROWS, COLS), BF16),
        fin=pltpu.VMEM((NY, ROWS, COLS), BF16),
        dx=pltpu.VMEM((NY, ROWS, COLS), BF16),
        dg=pltpu.VMEM((NZ, DH, COLS), BF16),
        du=pltpu.VMEM((NZ, DH, COLS), BF16),
        dd=pltpu.VMEM((NZ, DH, COLS), BF16),
        dpart=pltpu.VMEM((2, 2 * gathered, NZ * DH), BF16),
        dparts=pltpu.VMEM((NT, 2, 2 * gathered // NT, NZ * DH), BF16),
        dhid=pltpu.VMEM((2 * gathered // NT, NZ * DH), BF16),
        dhids=pltpu.VMEM((2 * gathered, NZ * DH), BF16),
        dacc=pltpu.VMEM((NC * NY, ROWS, COLS), BF16),
        dfin=pltpu.VMEM((NC * NY, ROWS, COLS), BF16),
        near=pltpu.SemaphoreType.REGULAR,
        wide=pltpu.SemaphoreType.REGULAR,
        loc=dma((16,)),
        s_hp=dma,
        r_hp=dma,
        s_wdn=dma,
        r_wdn=dma,
        s_rt=dma,
        r_rt=dma,
        s_sc=dma,
        r_sc=dma,
        s_x=dma,
        r_x=dma,
        s_dx=dma,
        r_dx=dma,
        s_dw=dma((3,)),
        r_dw=dma((3,)),
        s_z=dma,
        r_z=dma((nch,)),
        s_up=dma,
        r_up=dma((nch,)),
        s_ag=dma,
        r_ag=dma((nch,)),
        s_rz=dma,
        r_rz=dma,
        s_drs=dma,
        r_drs=dma,
        s_dag=dma,
        r_dag=dma,
        s_dy=dma,
        r_dy=dma,
        s_y=dma,
        r_y=dma,
    )


def kernel(
    tokens,
    positions,
    state,
    mix_gain,
    w_query,
    w_key,
    w_value,
    w_out,
    ffn_gain,
    branch_gate,
    dense_gate,
    dense_up,
    dense_down,
    routes,
    scores,
    expert_gate,
    expert_up,
    expert_down,
    freq,
    out,
    *scratch,
):
    m = types.SimpleNamespace(**dict(zip(scratch_table(), scratch)))
    ep = lax.axis_index("ep")
    t = lax.axis_index("tp")
    z, y, c = ep // 16, (ep // 2) % 8, ep % 2

    def at(a=0, b=0, dc=0, dt=0):
        to_z = lax.rem(z + a * c + b * (1 - c), NZ)
        to_y = lax.rem(y + a * (1 - c) + b * c, NY)
        return (to_z * 16 + to_y * 2 + lax.rem(c + dc, NC), lax.rem(t + dt, NT))

    def send(src, dst, s, r, dev):
        pltpu.make_async_remote_copy(
            src_ref=src, dst_ref=dst, send_sem=s, recv_sem=r, device_id=dev, device_id_type=MESH
        ).start()

    def wait(ref, sem):
        pltpu.make_async_copy(ref, ref, sem).wait()

    def block(d):
        return pl.ds(pl.multiple_of(lax.rem(t + d, NT) * COLS, COLS), COLS)

    def fetch(k, *pairs):
        for src, dst in pairs:
            pltpu.make_async_copy(src, dst, m.loc.at[k]).start()

    fetch(0, (tokens, m.tok))
    fetch(1, (mix_gain, m.mixg))
    fetch(2, (positions, m.pos))
    fetch(3, (freq, m.freq))
    fetch(
        4,
        *[
            (n, m.wqkv.at[:, pl.ds(HEAD * k, HEAD)])
            for k, n in enumerate((w_query, w_key, w_value))
        ],
    )
    fetch(5, (state, m.state))
    fetch(6, (w_out, m.wout))

    barrier = pltpu.get_barrier_semaphore()

    def greet(dz, dy, dx, core):
        to = lax.rem(z + dz, NZ) * 16 + lax.rem(y + dy, NY) * 2 + core
        pl.semaphore_signal(
            barrier, 1, device_id=(to, lax.rem(t + dx, NT)), device_id_type=MESH
        )

    for d in range(1, NT):
        greet(0, 0, d, 0)
    for d in range(1, NY):
        greet(0, d, 0, 1)
    for d in range(1, NZ):
        greet(d, 0, 0, 1)

    @pl.when(c == 0)
    def _():
        greet(0, 0, 0, 1)

    @pl.when(c == 1)
    def _():
        greet(0, 0, 0, 0)

    wait(m.tok, m.loc.at[0])
    wait(m.mixg, m.loc.at[1])
    tok = m.tok[...].astype(F32)
    scale = lax.rsqrt(jnp.mean(tok * tok, axis=1, keepdims=True) + EPS)
    gain = m.mixg[...]
    normed = jnp.concatenate(
        [
            (tok[:, 128 * j : 128 * j + 128] * scale * gain[j : j + 1]).astype(BF16)
            for j in range(WIDTH // 128)
        ],
        axis=1,
    )
    wait(m.pos, m.loc.at[2])
    wait(m.freq, m.loc.at[3])
    eye = lax.broadcasted_iota(jnp.int32, (ROWS, ROWS), 0) == lax.broadcasted_iota(
        jnp.int32, (ROWS, ROWS), 1
    )
    where = jnp.sum(jnp.where(eye, m.pos[...].astype(F32), 0.0), axis=1, keepdims=True)
    angle = where * m.freq[...]
    lane = lax.broadcasted_iota(jnp.int32, (ROWS, HEAD), 1)
    cosine = jnp.cos(angle)
    sine = jnp.where(lane < HEAD // 2, -jnp.sin(angle), jnp.sin(angle))
    wait(m.wqkv, m.loc.at[4])
    qkv = dot(normed, m.wqkv[...])
    query, key, value = (qkv[:, HEAD * k : HEAD * (k + 1)] for k in range(3))

    def rotate(v):
        return v * cosine + pltpu.roll(v, HEAD // 2, 1) * sine

    query = rotate(query)
    key = rotate(key) * HEAD**-0.5
    head = t.astype(F32)
    decay = 1.0 - jnp.exp2(jnp.full((1, HEAD), -5.0 - 5.0 * head / (NT - 1), F32))
    columns = query.T
    wait(m.state, m.loc.at[5])
    for s in range(ROWS):
        m.ret[pl.ds(s, 1), :] = jnp.sum(
            m.state[s] * columns[:, s : s + 1], axis=0, keepdims=True
        )
    retrieved = m.ret[...] * decay + jnp.sum(query * key, axis=1, keepdims=True) * value
    retrieved = retrieved * lax.rsqrt(
        jnp.mean(retrieved * retrieved, axis=1, keepdims=True) + EPS
    )
    fetch(7, (ffn_gain, m.ffng))
    fetch(8, (routes, m.rt.at[0]))
    fetch(9, (scores, m.sc.at[0]))
    fetch(10, (expert_down.at[:, block(0)], m.wdn.at[0]))
    for k, (src, dst) in enumerate(((dense_gate, m.dg), (dense_up, m.du), (dense_down, m.dd))):
        fetch(11 + k, (src, dst.at[0]))
    fetch(14, (branch_gate, m.bgate))
    fetch(
        15,
        *[
            (n.at[block(d)], m.wgu.at[pl.ds(COLS * d, COLS), pl.ds(HID * k, HID)])
            for d in range(NT)
            for k, n in enumerate((expert_gate, expert_up))
        ],
    )
    wait(m.wout, m.loc.at[6])
    m.hp[0] = dot(retrieved.astype(BF16), m.wout[...]).astype(BF16)

    gathered = NY * ROWS
    quarter = 2 * gathered // NT
    left = pl.ds(0, 2 * COLS)
    right = pl.ds(2 * COLS, 2 * COLS)
    dense = (m.dg, m.du, m.dd)

    def part(d):
        return pl.ds(pl.multiple_of(lax.rem(t + d, NT) * quarter, quarter), quarter)

    def chunk_of(spot):
        return [n for n, (lo, hi) in enumerate(CHUNKS) if lo <= spot < hi][0]

    def spread(k):
        src = (dense_gate, dense_up, dense_down)[k]
        for d in FAR:
            send(src, dense[k].at[NZ - d], m.s_dw.at[k], m.r_dw.at[k], at(b=d))

    def spread_routes():
        for d in FAR:
            send(routes, m.rt.at[NY - d], m.s_rt, m.r_rt, at(a=d))
            send(scores, m.sc.at[NY - d], m.s_sc, m.r_sc, at(a=d))

    def split_down():
        for d in (2, 1, 3):
            send(expert_down.at[:, block(d)], m.wdn.at[NT - d], m.s_wdn, m.r_wdn, at(dt=d))

    def mix():
        for d in (2, 1, 3):
            send(m.hp.at[0], m.hp.at[NT - d], m.s_hp, m.r_hp, at(dt=d))

    def gather():
        wait(m.ffng, m.loc.at[7])
        wait(m.hp.at[pl.ds(1, NT - 1)], m.r_hp)
        after = tok
        for d in range(NT):
            after = after + m.hp[d].astype(F32)
        m.after[...] = after
        scale = lax.rsqrt(jnp.mean(after * after, axis=1, keepdims=True) + EPS)
        gain = m.ffng[...]
        for j in range(WIDTH // 128):
            m.ffn[:, 128 * j : 128 * j + 128] = (
                after[:, 128 * j : 128 * j + 128] * scale * gain[j : j + 1]
            ).astype(BF16)
        for d in range(2):
            m.x[0, :, COLS * d : COLS * (d + 1)] = m.ffn[:, block(d)]
        for d in FAR:
            send(m.x.at[0], m.x.at[NY - d], m.s_x, m.r_x, at(a=d))

    def gather_other():
        for d in FAR + (0,):
            send(
                m.x.at[0, :, pl.ds(0, COLS)],
                m.dx.at[(NY - d) % NY],
                m.s_dx,
                m.r_dx,
                at(b=d, dc=1),
            )

    def assign():
        wait(m.rt.at[0], m.loc.at[8])
        wait(m.sc.at[0], m.loc.at[9])
        wait(m.rt.at[pl.ds(1, NY - 1)], m.r_rt)
        wait(m.sc.at[pl.ds(1, NY - 1)], m.r_sc)
        chosen = jnp.concatenate([m.rt[d] for d in range(NY)], axis=1)
        scored = jnp.concatenate([m.sc[d] for d in range(NY)], axis=1)
        shares = scored / jnp.sum(scored, axis=0, keepdims=True)
        k = lax.broadcasted_iota(jnp.int32, (NE, 128), 0)
        lane = lax.broadcasted_iota(jnp.int32, (NE, 128), 1)
        expert = (
            ((z + (k // 2) * (1 - c)) & 7) * 16 + ((y + (k // 2) * c) & 7) * 2 + ((c + k) & 1)
        )
        named = jnp.zeros((NE, 128), F32)
        share = jnp.zeros((NE, 128), F32)
        for n in range(6):
            hit = chosen[n : n + 1] == expert
            named = jnp.where(hit, 1.0, named)
            share = jnp.where(hit, shares[n : n + 1], share)
        a = lax.broadcasted_iota(jnp.int32, (128, 128), 0)
        b = lax.broadcasted_iota(jnp.int32, (128, 128), 1)
        ahead = jnp.where((a // ROWS == b // ROWS) & (a < b), 1.0, 0.0).astype(BF16)
        rank = dot(named.astype(BF16), ahead)
        code = jnp.where(named > 0.5, rank + (2 * (lane // ROWS)).astype(F32), -1.0)
        slot = lax.broadcasted_iota(jnp.int32, (ROWS, 128), 0).astype(F32)
        for n in range(NE):
            hit = code[n : n + 1] == slot
            m.place[pl.ds(ROWS * n, ROWS), :] = jnp.where(hit, 1.0, 0.0).astype(BF16)
            m.weigh[pl.ds(ROWS * n, ROWS), :] = jnp.where(hit, share[n : n + 1], 0.0).astype(BF16)

    def dispatch():
        wait(m.x.at[pl.ds(1, NY - 1)], m.r_x)
        m.slots[...] = (
            dot(m.place[...], m.x[...].reshape(NY * ROWS, 2 * COLS))
            .astype(BF16)
            .reshape(NE, ROWS, 2 * COLS)
        )
        for spot, d in enumerate(ORDER):
            for e in range(NC):
                k = NC * ((NZ - d) % NZ) + e
                if d or e:
                    send(
                        m.slots.at[k],
                        m.got.at[NC * spot + e, :, left],
                        m.s_z,
                        m.r_z.at[chunk_of(spot)],
                        at(b=(NZ - d) % NZ, dc=e),
                    )
                else:
                    m.got[NC * spot, :, left] = m.slots[k]

    def trade(n):
        if n == 0:
            wait(m.wgu, m.loc.at[15])
        lo, hi = CHUNKS[n]
        some = pl.ds(NC * lo, NC * (hi - lo))
        fresh = pl.ds(NC * lo, NC * (hi - lo) - (lo <= ORDER.index(0) < hi))
        wait(m.got.at[fresh, :, left], m.r_z.at[n])
        for k, d in ((0, 1), (1, 3)):
            send(
                m.got.at[some, :, pl.ds(COLS * k, COLS)],
                m.got.at[some, :, pl.ds(COLS * (3 - k), COLS)],
                m.s_up,
                m.r_up.at[n],
                at(dt=d),
            )
        size = NC * ROWS * (hi - lo)
        m.half[pl.ds(NC * ROWS * lo, size)] = dot(
            m.got[NC * lo : NC * hi, :, 0 : 2 * COLS].reshape(size, 2 * COLS),
            m.wgu[0 : 2 * COLS],
        )

    def hide(n):
        lo, hi = CHUNKS[n]
        size = NC * ROWS * (hi - lo)
        span = pl.ds(NC * ROWS * lo, size)
        wait(m.got.at[pl.ds(NC * lo, NC * (hi - lo)), :, right], m.r_up.at[n])
        total = m.half[span] + dot(
            m.got[NC * lo : NC * hi, :, 2 * COLS :].reshape(size, 2 * COLS),
            m.wgu[2 * COLS :],
        )
        pre = total[:, :HID]
        hidden = (pre / (1.0 + jnp.exp(-pre)) * total[:, HID:]).astype(BF16)
        m.hid[span] = hidden
        m.hids[span, 0:HID] = hidden
        for d in (2, 1, 3):
            send(
                m.hid.at[span],
                m.hids.at[span, pl.ds(HID * (NT - d), HID)],
                m.s_ag,
                m.r_ag.at[n],
                at(dt=d),
            )

    def answer(n):
        if n == 0:
            wait(m.wdn.at[0], m.loc.at[10])
            wait(m.wdn.at[pl.ds(1, NT - 1)], m.r_wdn)
        lo, hi = CHUNKS[n]
        size = NC * ROWS * (hi - lo)
        span = pl.ds(NC * ROWS * lo, size)
        wait(m.hids.at[span, pl.ds(HID, (NT - 1) * HID)], m.r_ag.at[n])
        m.rows[NC * lo : NC * hi] = (
            dot(m.hids[span], m.wdn[...].reshape(NT * HID, COLS))
            .astype(BF16)
            .reshape(NC * (hi - lo), ROWS, COLS)
        )
        for spot in range(lo, hi):
            d = ORDER[spot]
            for e in range(NC):
                if d or e:
                    send(
                        m.rows.at[NC * spot + e],
                        m.back.at[NC * ((NZ - d) % NZ) + e],
                        m.s_rz,
                        m.r_rz,
                        at(a=d, dc=1) if e else at(b=d),
                    )
                else:
                    m.back[0] = m.rows[NC * spot]

    def dense_in():
        wait(m.dx, m.r_dx)
        for k in range(2):
            wait(dense[k].at[0], m.loc.at[11 + k])
            wait(dense[k].at[pl.ds(1, NZ - 1)], m.r_dw.at[k])
            weights = dense[k][...].reshape(NZ * DH, COLS)
            m.dpart[k, 0:gathered] = dot_nt(
                m.x[:, :, 0:COLS].reshape(gathered, COLS), weights
            ).astype(BF16)
            m.dpart[k, gathered:] = dot_nt(m.dx[...].reshape(gathered, COLS), weights).astype(BF16)
        for d in (2, 1, 3):
            send(m.dpart.at[:, part(d)], m.dparts.at[NT - d], m.s_drs, m.r_drs, at(dt=d))

    def dense_hide():
        wait(m.dparts.at[pl.ds(1, NT - 1)], m.r_drs)
        pre = m.dpart[0, part(0)].astype(F32)
        up = m.dpart[1, part(0)].astype(F32)
        for d in range(1, NT):
            pre = pre + m.dparts[d, 0].astype(F32)
            up = up + m.dparts[d, 1].astype(F32)
        dhidden = (pre / (1.0 + jnp.exp(-pre)) * up).astype(BF16)
        m.dhid[...] = dhidden
        m.dhids[part(0)] = dhidden
        for d in (2, 1, 3):
            send(m.dhid, m.dhids.at[part(0)], m.s_dag, m.r_dag, at(dt=d))

    def dense_out():
        wait(dense[2].at[0], m.loc.at[13])
        wait(dense[2].at[pl.ds(1, NZ - 1)], m.r_dw.at[2])
        wait(m.dhids.at[pl.ds(0, 2 * gathered - quarter)], m.r_dag)
        m.dacc[...] = (
            dot(m.dhids[...], m.dd[...].reshape(NZ * DH, COLS))
            .astype(BF16)
            .reshape(NC * NY, ROWS, COLS)
        )
        for d in FAR + (0,):
            for e in range(NC):
                if d or e:
                    send(
                        m.dacc.at[NY * e + d],
                        m.dfin.at[NY * e + (NY - d) % NY],
                        m.s_dy,
                        m.r_dy,
                        at(a=d, dc=e),
                    )

    def finish():
        wait(m.back.at[pl.ds(1, NE - 1)], m.r_rz)
        both = dot_tn(m.weigh[...], m.back[...].reshape(NE * ROWS, COLS))
        m.acc[...] = both.astype(BF16).reshape(NY, ROWS, COLS)
        for d in FAR:
            send(m.acc.at[d], m.fin.at[NY - d], m.s_y, m.r_y, at(a=d))
        wait(m.bgate, m.loc.at[14])
        gate = m.bgate[...].astype(F32)
        branch = jnp.zeros((ROWS, 128), F32)
        for j in range(WIDTH // 128):
            branch = branch + m.ffn[:, 128 * j : 128 * j + 128].astype(F32) * gate[j : j + 1]
        branch = jnp.sum(branch, axis=1, keepdims=True)
        branch = 1.0 / (1.0 + jnp.exp(-branch))
        wait(m.dfin.at[pl.ds(1, NC * NY - 1)], m.r_dy)
        total = m.dacc[0].astype(F32)
        for d in range(1, NC * NY):
            total = total + m.dfin[d].astype(F32)
        total = m.after[:, block(0)] + branch * total + m.acc[0].astype(F32)
        wait(m.fin.at[pl.ds(1, NY - 1)], m.r_y)
        for d in range(1, NY):
            total = total + m.fin[d].astype(F32)
        out[...] = total.astype(BF16)

    def meet(core, count, sem):
        @pl.when(c == core)
        def _():
            pl.semaphore_wait(barrier, count)
            pl.semaphore_signal(sem, 1, device_id=at(dc=1), device_id_type=MESH)

        @pl.when(c != core)
        def _():
            pl.semaphore_wait(sem, 1)

    meet(0, NC * (NT - 1) + 1, m.near)
    mix()
    meet(1, NC * (NY - 1 + NZ - 1) + 1, m.wide)
    spread_routes()
    spread(0)
    spread(1)
    gather()
    gather_other()
    split_down()
    assign()
    dispatch()
    dense_in()
    trade(0)
    trade(1)
    trade(2)
    trade(3)
    spread(2)
    hide(0)
    hide(1)
    hide(2)
    hide(3)
    dense_hide()
    answer(0)
    answer(1)
    answer(2)
    answer(3)
    dense_out()
    finish()

    wait(m.hp.at[pl.ds(1, NT - 1)], m.s_hp)
    wait(m.rt.at[pl.ds(1, NY - 1)], m.s_rt)
    wait(m.sc.at[pl.ds(1, NY - 1)], m.s_sc)
    wait(m.wdn.at[pl.ds(1, NT - 1)], m.s_wdn)
    wait(m.x.at[pl.ds(1, NY - 1)], m.s_x)
    wait(m.dx, m.s_dx)
    for k in range(3):
        wait(dense[k].at[pl.ds(1, NZ - 1)], m.s_dw.at[k])
    wait(m.got.at[pl.ds(1, NE - 1), :, left], m.s_z)
    wait(m.got.at[:, :, right], m.s_up)
    wait(m.hids.at[:, pl.ds(HID, (NT - 1) * HID)], m.s_ag)
    wait(m.dparts.at[pl.ds(1, NT - 1)], m.s_drs)
    wait(m.dhids.at[pl.ds(0, 2 * gathered - quarter)], m.s_dag)
    wait(m.back.at[pl.ds(1, NE - 1)], m.s_rz)
    wait(m.dfin.at[pl.ds(1, NC * NY - 1)], m.s_dy)
    wait(m.fin.at[pl.ds(1, NY - 1)], m.s_y)


def on_device(
    tokens,
    positions,
    state,
    mix_gain,
    w_query,
    w_key,
    w_value,
    w_out,
    ffn_gain,
    branch_gate,
    dense_gate,
    dense_up,
    dense_down,
    routes,
    route_scores,
    expert_gate,
    expert_up,
    expert_down,
):
    half = HEAD // 2
    inverse = 10000.0 ** -(np.arange(half, dtype=np.float64) / (half - 1))
    freq = jnp.asarray(np.concatenate([inverse, inverse])[None], F32)
    args = (
        tokens,
        positions.reshape(1, ROWS),
        state.reshape(ROWS, HEAD, HEAD),
        mix_gain.reshape(WIDTH // 128, 128),
        w_query,
        w_key,
        w_value,
        w_out,
        ffn_gain.reshape(WIDTH // 128, 128),
        branch_gate.reshape(WIDTH // 128, 128),
        dense_gate.T,
        dense_up.T,
        dense_down,
        routes.T,
        route_scores.T,
        expert_gate.reshape(WIDTH, HID),
        expert_up.reshape(WIDTH, HID),
        expert_down.reshape(HID, WIDTH),
        freq,
    )
    return pl.pallas_call(
        kernel,
        name="layer",
        out_shape=pltpu.VMEM((ROWS, COLS), BF16),
        in_specs=[pl.BlockSpec(memory_space=pltpu.HBM)] * len(args),
        out_specs=pl.BlockSpec(memory_space=pltpu.VMEM),
        scratch_shapes=list(scratch_table().values()),
        compiler_params=pltpu.CompilerParams(
            collective_id=0, has_side_effects=True, vmem_limit_bytes=60 * 1024 * 1024
        ),
    )(*args)


def solution(mesh):
    placed = (
        P("ep", None),
        P("ep"),
        P("ep", "tp", None, None),
        P(),
        P(None, "tp"),
        P(None, "tp"),
        P(None, "tp"),
        P("tp", None),
        P(),
        P(),
        P("tp", "ep"),
        P("tp", "ep"),
        P("ep", "tp"),
        P("ep", None),
        P("ep", None),
        P("ep", None, "tp"),
        P("ep", None, "tp"),
        P("ep", "tp", None),
    )
    return jax.shard_map(
        on_device, mesh=mesh, in_specs=placed, out_specs=P("ep", "tp"), check_vma=False
    )
```

```python
import types

import jax
import jax.numpy as jnp
import numpy as np
from jax import lax
from jax.experimental import pallas as pl
from jax.experimental.pallas import tpu as pltpu
from jax.sharding import PartitionSpec as P

EPS = 1e-06
MESH = pl.DeviceIdType.MESH
F32 = jnp.float32
BF16 = jnp.bfloat16
NZ, NY, NC, NT = 8, 8, 2, 4
ROWS = 16
WIDTH = 2048
HEAD = 128
COLS = WIDTH // NT
HID = 128
DH = 32
NE = NZ * NC
HALF = NZ // 2
WAVES = 2
UNIT = 8
FAR = (4, 3, 5, 2, 6, 1, 7)


def dot(a, b):
    return jnp.dot(a, b, preferred_element_type=F32)


def dot_nt(a, b):
    return lax.dot_general(a, b, (((1,), (1,)), ((), ())), preferred_element_type=F32)


def dot_tn(a, b):
    return lax.dot_general(a, b, (((0,), (0,)), ((), ())), preferred_element_type=F32)


def scratch_table():
    dma = pltpu.SemaphoreType.DMA
    gathered = NY * ROWS
    wave = NE * UNIT
    return dict(
        tok=pltpu.VMEM((ROWS, WIDTH), BF16),
        pos=pltpu.VMEM((1, ROWS), jnp.int32),
        state=pltpu.VMEM((ROWS, HEAD, HEAD), F32),
        mixg=pltpu.VMEM((WIDTH // 128, 128), F32),
        wqkv=pltpu.VMEM((WIDTH, 3 * HEAD), BF16),
        wout=pltpu.VMEM((HEAD, WIDTH), BF16),
        ffng=pltpu.VMEM((WIDTH // 128, 128), F32),
        bgate=pltpu.VMEM((WIDTH // 128, 128), BF16),
        freq=pltpu.VMEM((1, 128), F32),
        hp=pltpu.VMEM((NT, ROWS, WIDTH), BF16),
        after=pltpu.VMEM((ROWS, WIDTH), F32),
        ffn=pltpu.VMEM((ROWS, WIDTH), BF16),
        x=pltpu.VMEM((NY, ROWS, 2 * COLS), BF16),
        rt=pltpu.VMEM((NY, 6, ROWS), jnp.int32),
        sc=pltpu.VMEM((NY, 6, ROWS), F32),
        place=pltpu.VMEM((2, wave, gathered // 2), BF16),
        weigh=pltpu.VMEM((2, wave, gathered // 2), BF16),
        slots=pltpu.VMEM((2, NE, UNIT, 2 * COLS), BF16),
        got=pltpu.VMEM((WAVES, NE, UNIT, WIDTH), BF16),
        wgu=pltpu.VMEM((WIDTH, 2 * HID), BF16),
        wdn=pltpu.VMEM((NT, HID, COLS), BF16),
        half=pltpu.VMEM((WAVES, wave, 2 * HID), F32),
        hid=pltpu.VMEM((WAVES, wave, HID), BF16),
        hids=pltpu.VMEM((WAVES, wave, NT * HID), BF16),
        rows=pltpu.VMEM((WAVES, NE, UNIT, COLS), BF16),
        back=pltpu.VMEM((2, NE, UNIT, COLS), BF16),
        acc=pltpu.VMEM((NY, ROWS, COLS), BF16),
        fin=pltpu.VMEM((NY, ROWS, COLS), BF16),
        dx=pltpu.VMEM((NY, ROWS, COLS), BF16),
        dg=pltpu.VMEM((NZ, DH, COLS), BF16),
        du=pltpu.VMEM((NZ, DH, COLS), BF16),
        dd=pltpu.VMEM((NZ, DH, COLS), BF16),
        dpart=pltpu.VMEM((2, 2 * gathered, NZ * DH), BF16),
        dparts=pltpu.VMEM((NT, 2, 2 * gathered // NT, NZ * DH), BF16),
        dhid=pltpu.VMEM((2 * gathered // NT, NZ * DH), BF16),
        dhids=pltpu.VMEM((2 * gathered, NZ * DH), BF16),
        dacc=pltpu.VMEM((NC * NY, ROWS, COLS), BF16),
        dfin=pltpu.VMEM((NC * NY, ROWS, COLS), BF16),
        near=pltpu.SemaphoreType.REGULAR,
        wide=pltpu.SemaphoreType.REGULAR,
        loc=dma((16,)),
        s_hp=dma,
        r_hp=dma,
        s_wdn=dma,
        r_wdn=dma,
        s_rt=dma,
        r_rt=dma,
        s_sc=dma,
        r_sc=dma,
        s_x=dma,
        r_x=dma((2,)),
        s_dx=dma,
        r_dx=dma,
        s_dw=dma((3,)),
        r_dw=dma((3,)),
        s_z=dma,
        r_z=dma((2 * WAVES,)),
        s_up=dma,
        r_up=dma((2 * WAVES,)),
        s_ag=dma,
        r_ag=dma((2 * WAVES,)),
        s_rz=dma,
        r_rz=dma((2,)),
        s_drs=dma,
        r_drs=dma,
        s_dag=dma,
        r_dag=dma,
        s_dy=dma,
        r_dy=dma,
        s_y=dma,
        r_y=dma,
    )


def kernel(
    tokens,
    positions,
    state,
    mix_gain,
    w_query,
    w_key,
    w_value,
    w_out,
    ffn_gain,
    branch_gate,
    dense_gate,
    dense_up,
    dense_down,
    routes,
    scores,
    expert_gate,
    expert_up,
    expert_down,
    freq,
    out,
    *scratch,
):
    m = types.SimpleNamespace(**dict(zip(scratch_table(), scratch)))
    ep = lax.axis_index("ep")
    t = lax.axis_index("tp")
    z, y, c = ep // 16, (ep // 2) % 8, ep % 2

    def at(a=0, b=0, dc=0, dt=0):
        to_z = lax.rem(z + a * c + b * (1 - c), NZ)
        to_y = lax.rem(y + a * (1 - c) + b * c, NY)
        return (to_z * 16 + to_y * 2 + lax.rem(c + dc, NC), lax.rem(t + dt, NT))

    def send(src, dst, s, r, dev):
        pltpu.make_async_remote_copy(
            src_ref=src, dst_ref=dst, send_sem=s, recv_sem=r, device_id=dev, device_id_type=MESH
        ).start()

    def wait(ref, sem):
        pltpu.make_async_copy(ref, ref, sem).wait()

    def block(d):
        return pl.ds(pl.multiple_of(lax.rem(t + d, NT) * COLS, COLS), COLS)

    near_half = z // HALF
    mine_a = y * (1 - c) + z * c
    mine_b = z * (1 - c) + y * c

    def fetch(k, *pairs):
        for src, dst in pairs:
            pltpu.make_async_copy(src, dst, m.loc.at[k]).start()

    fetch(0, (tokens, m.tok))
    fetch(1, (mix_gain, m.mixg))
    fetch(2, (positions, m.pos))
    fetch(3, (freq, m.freq))
    fetch(
        4,
        *[
            (n, m.wqkv.at[:, pl.ds(HEAD * k, HEAD)])
            for k, n in enumerate((w_query, w_key, w_value))
        ],
    )
    fetch(5, (state, m.state))
    fetch(6, (w_out, m.wout))

    barrier = pltpu.get_barrier_semaphore()

    def greet(dz, dy, dx, core):
        to = lax.rem(z + dz, NZ) * 16 + lax.rem(y + dy, NY) * 2 + core
        pl.semaphore_signal(
            barrier, 1, device_id=(to, lax.rem(t + dx, NT)), device_id_type=MESH
        )

    for d in range(1, NT):
        greet(0, 0, d, 0)
    for d in range(1, NY):
        greet(0, d, 0, 1)
    for d in range(1, NZ):
        greet(d, 0, 0, 1)

    @pl.when(c == 0)
    def _():
        greet(0, 0, 0, 1)

    @pl.when(c == 1)
    def _():
        greet(0, 0, 0, 0)

    wait(m.tok, m.loc.at[0])
    wait(m.mixg, m.loc.at[1])
    tok = m.tok[...].astype(F32)
    scale = lax.rsqrt(jnp.mean(tok * tok, axis=1, keepdims=True) + EPS)
    gain = m.mixg[...]
    normed = jnp.concatenate(
        [
            (tok[:, 128 * j : 128 * j + 128] * scale * gain[j : j + 1]).astype(BF16)
            for j in range(WIDTH // 128)
        ],
        axis=1,
    )
    wait(m.pos, m.loc.at[2])
    wait(m.freq, m.loc.at[3])
    eye = lax.broadcasted_iota(jnp.int32, (ROWS, ROWS), 0) == lax.broadcasted_iota(
        jnp.int32, (ROWS, ROWS), 1
    )
    where = jnp.sum(jnp.where(eye, m.pos[...].astype(F32), 0.0), axis=1, keepdims=True)
    angle = where * m.freq[...]
    lane = lax.broadcasted_iota(jnp.int32, (ROWS, HEAD), 1)
    cosine = jnp.cos(angle)
    sine = jnp.where(lane < HEAD // 2, -jnp.sin(angle), jnp.sin(angle))
    wait(m.wqkv, m.loc.at[4])
    qkv = dot(normed, m.wqkv[...])
    query, key, value = (qkv[:, HEAD * k : HEAD * (k + 1)] for k in range(3))

    def rotate(v):
        return v * cosine + pltpu.roll(v, HEAD // 2, 1) * sine

    query = rotate(query)
    key = rotate(key) * HEAD**-0.5
    head = t.astype(F32)
    decay = 1.0 - jnp.exp2(jnp.full((1, HEAD), -5.0 - 5.0 * head / (NT - 1), F32))
    row = lax.broadcasted_iota(jnp.int32, (ROWS, HEAD), 0)
    apart = jnp.concatenate(
        [jnp.where(row == s, query, 0.0).astype(BF16) for s in range(ROWS)], axis=1
    )
    wait(m.state, m.loc.at[5])
    held = dot(apart, m.state[...].reshape(ROWS * HEAD, HEAD).astype(BF16))
    retrieved = held * decay + jnp.sum(query * key, axis=1, keepdims=True) * value
    retrieved = retrieved * lax.rsqrt(
        jnp.mean(retrieved * retrieved, axis=1, keepdims=True) + EPS
    )
    fetch(7, (ffn_gain, m.ffng))
    fetch(8, (routes, m.rt.at[mine_a]))
    fetch(9, (scores, m.sc.at[mine_a]))
    fetch(10, (expert_down.at[:, block(0)], m.wdn.at[0]))
    for k, (src, dst) in enumerate(((dense_gate, m.dg), (dense_up, m.du), (dense_down, m.dd))):
        fetch(11 + k, (src, dst.at[0]))
    fetch(14, (branch_gate, m.bgate))
    fetch(
        15,
        *[
            (n.at[block(d)], m.wgu.at[pl.ds(COLS * d, COLS), pl.ds(HID * k, HID)])
            for d in range(NT)
            for k, n in enumerate((expert_gate, expert_up))
        ],
    )
    wait(m.wout, m.loc.at[6])
    m.hp[0] = dot(retrieved.astype(BF16), m.wout[...]).astype(BF16)

    gathered = NY * ROWS
    quarter = 2 * gathered // NT
    left = pl.ds(0, 2 * COLS)
    right = pl.ds(2 * COLS, 2 * COLS)
    dense = (m.dg, m.du, m.dd)

    def part(d):
        return pl.ds(pl.multiple_of(lax.rem(t + d, NT) * quarter, quarter), quarter)

    def spread(k):
        src = (dense_gate, dense_up, dense_down)[k]
        for d in FAR:
            send(src, dense[k].at[NZ - d], m.s_dw.at[k], m.r_dw.at[k], at(b=d))

    def spread_routes():
        for d in FAR:
            send(routes, m.rt.at[mine_a], m.s_rt, m.r_rt, at(a=d))
            send(scores, m.sc.at[mine_a], m.s_sc, m.r_sc, at(a=d))

    def split_down():
        for d in (2, 1, 3):
            send(expert_down.at[:, block(d)], m.wdn.at[NT - d], m.s_wdn, m.r_wdn, at(dt=d))

    def mix():
        for d in (2, 1, 3):
            send(m.hp.at[0], m.hp.at[NT - d], m.s_hp, m.r_hp, at(dt=d))

    def gather():
        wait(m.ffng, m.loc.at[7])
        wait(m.hp.at[pl.ds(1, NT - 1)], m.r_hp)
        after = tok
        for d in range(NT):
            after = after + m.hp[d].astype(F32)
        m.after[...] = after
        scale = lax.rsqrt(jnp.mean(after * after, axis=1, keepdims=True) + EPS)
        gain = m.ffng[...]
        for j in range(WIDTH // 128):
            m.ffn[:, 128 * j : 128 * j + 128] = (
                after[:, 128 * j : 128 * j + 128] * scale * gain[j : j + 1]
            ).astype(BF16)
        for d in range(2):
            m.x[mine_a, :, COLS * d : COLS * (d + 1)] = m.ffn[:, block(d)]
        for d in FAR:
            send(m.x.at[mine_a], m.x.at[mine_a], m.s_x, m.r_x.at[mine_a // HALF], at(a=d))

    def gather_other():
        for d in FAR + (0,):
            send(
                m.x.at[mine_a, :, pl.ds(0, COLS)],
                m.dx.at[mine_b],
                m.s_dx,
                m.r_dx,
                at(b=d, dc=1),
            )

    def assign():
        wait(m.rt.at[0], m.loc.at[8])
        wait(m.sc.at[0], m.loc.at[9])
        wait(m.rt.at[pl.ds(1, NY - 1)], m.r_rt)
        wait(m.sc.at[pl.ds(1, NY - 1)], m.r_sc)
        tokens_h = HALF * ROWS
        k = lax.broadcasted_iota(jnp.int32, (NE, tokens_h), 0)
        lane = lax.broadcasted_iota(jnp.int32, (NE, tokens_h), 1)
        expert = ((k // 2) * (1 - c) + z * c) * 16 + ((k // 2) * c + y * (1 - c)) * 2 + (k & 1)
        a = lax.broadcasted_iota(jnp.int32, (tokens_h, tokens_h), 0)
        b = lax.broadcasted_iota(jnp.int32, (tokens_h, tokens_h), 1)
        ahead = jnp.where((a // ROWS == b // ROWS) & (a < b), 1.0, 0.0).astype(BF16)
        slot = lax.broadcasted_iota(jnp.int32, (UNIT, tokens_h), 0).astype(F32)
        for h in range(2):
            some = range(HALF * h, HALF * (h + 1))
            chosen = jnp.concatenate([m.rt[d] for d in some], axis=1)
            scored = jnp.concatenate([m.sc[d] for d in some], axis=1)
            shares = scored / jnp.sum(scored, axis=0, keepdims=True)
            named = jnp.zeros((NE, tokens_h), F32)
            share = jnp.zeros((NE, tokens_h), F32)
            for n in range(6):
                hit = chosen[n : n + 1] == expert
                named = jnp.where(hit, 1.0, named)
                share = jnp.where(hit, shares[n : n + 1], share)
            rank = dot(named.astype(BF16), ahead)
            code = jnp.where(named > 0.5, rank + (2 * (lane // ROWS)).astype(F32), -1.0)
            for n in range(NE):
                hit = code[n : n + 1] == slot
                at_n = pl.ds(UNIT * n, UNIT)
                m.place[h, at_n, :] = jnp.where(hit, 1.0, 0.0).astype(BF16)
                m.weigh[h, at_n, :] = jnp.where(hit, share[n : n + 1], 0.0).astype(BF16)

    def emit(h):
        inside = mine_a // HALF == h

        @pl.when(inside)
        def _():
            wait(m.x.at[pl.ds(0, HALF - 1)], m.r_x.at[h])

        @pl.when(jnp.logical_not(inside))
        def _():
            wait(m.x.at[pl.ds(0, HALF)], m.r_x.at[h])

        m.slots[h] = (
            dot(
                m.place[h],
                m.x[HALF * h : HALF * (h + 1)].reshape(HALF * ROWS, 2 * COLS),
            )
            .astype(BF16)
            .reshape(NE, UNIT, 2 * COLS)
        )
        wave = c * h + (1 - c) * near_half
        for d in FAR + (0,):
            spot = c * (NE // 2 + (NZ - d) % NZ) + (1 - c) * (2 * ((NZ - d) % HALF) + h)
            for e in range(NC):
                k = lax.rem(mine_b + d, NZ) * 2 + lax.rem(c + e, NC)
                if d or e:
                    send(
                        m.slots.at[h, k],
                        m.got.at[wave, spot, :, left],
                        m.s_z,
                        m.r_z.at[2 * wave + c],
                        at(b=d, dc=e),
                    )
                else:
                    m.got[wave, spot, :, left] = m.slots[h, k]

    def up_ready():
        wait(m.wgu, m.loc.at[15])

    def down_ready():
        wait(m.wdn.at[0], m.loc.at[10])
        wait(m.wdn.at[pl.ds(1, NT - 1)], m.r_wdn)

    def trade(w, k):
        n, begin, count = 2 * w + k, NE // 2 * k, NE // 2
        own = (near_half == w) & (c == 0) if k == 0 else c == 1

        @pl.when(own)
        def _():
            wait(m.got.at[w, pl.ds(begin, count - (2 - k)), :, left], m.r_z.at[n])

        @pl.when(jnp.logical_not(own))
        def _():
            wait(m.got.at[w, pl.ds(begin, count), :, left], m.r_z.at[n])

        some = pl.ds(begin, count)
        for j, d in ((0, 1), (1, 3)):
            send(
                m.got.at[w, some, :, pl.ds(COLS * j, COLS)],
                m.got.at[w, some, :, pl.ds(COLS * (3 - j), COLS)],
                m.s_up,
                m.r_up.at[n],
                at(dt=d),
            )
        m.half[w, pl.ds(UNIT * begin, UNIT * count)] = dot(
            m.got[w, begin : begin + count, :, 0 : 2 * COLS].reshape(count * UNIT, 2 * COLS),
            m.wgu[0 : 2 * COLS],
        )

    def hide(w, k):
        n, begin, count = 2 * w + k, NE // 2 * k, NE // 2
        span = pl.ds(UNIT * begin, UNIT * count)
        wait(m.got.at[w, pl.ds(begin, count), :, right], m.r_up.at[n])
        total = m.half[w, span] + dot(
            m.got[w, begin : begin + count, :, 2 * COLS :].reshape(count * UNIT, 2 * COLS),
            m.wgu[2 * COLS :],
        )
        pre = total[:, :HID]
        hidden = (pre / (1.0 + jnp.exp(-pre)) * total[:, HID:]).astype(BF16)
        m.hid[w, span] = hidden
        m.hids[w, span, 0:HID] = hidden
        for d in (2, 1, 3):
            send(
                m.hid.at[w, span],
                m.hids.at[w, span, pl.ds(HID * (NT - d), HID)],
                m.s_ag,
                m.r_ag.at[n],
                at(dt=d),
            )

    def answer(w, k):
        n, begin, count = 2 * w + k, NE // 2 * k, NE // 2
        span = pl.ds(UNIT * begin, UNIT * count)
        wait(m.hids.at[w, span, pl.ds(HID, (NT - 1) * HID)], m.r_ag.at[n])
        m.rows[w, begin : begin + count] = (
            dot(m.hids[w, span], m.wdn[...].reshape(NT * HID, COLS))
            .astype(BF16)
            .reshape(count, UNIT, COLS)
        )

        def reply(spot, to, h, k):
            send(m.rows.at[w, spot], m.back.at[h, k], m.s_rz, m.r_rz.at[h], (to, t))

        for d in (2, 1, 3, 0) if k == 0 else ():
            to = (HALF * w + lax.rem(z + d, HALF)) * 16 + y * 2
            for h in range(2):
                spot, e = 2 * d + h, z * 2 + c
                if d:
                    reply(spot, to, h, e)
                    continue
                own = (c == 0) & (near_half == w)

                @pl.when(jnp.logical_not(own))
                def _(spot=spot, to=to, h=h, e=e):
                    reply(spot, to, h, e)

                @pl.when(own)
                def _(spot=spot, h=h, e=e):
                    m.back[h, e] = m.rows[w, spot]

        for d in FAR + (0,) if k == 1 else ():
            to = z * 16 + lax.rem(y + d, NY) * 2 + 1
            spot, e = NE // 2 + d, y * 2 + c
            if d:
                reply(spot, to, w, e)
                continue

            @pl.when(c == 0)
            def _(spot=spot, to=to, e=e):
                reply(spot, to, w, e)

            @pl.when(c == 1)
            def _(spot=spot, e=e):
                m.back[w, e] = m.rows[w, spot]

    def combine(h):
        wait(m.back.at[h, pl.ds(0, NE - 1)], m.r_rz.at[h])
        both = dot_tn(m.weigh[h], m.back[h].reshape(NE * UNIT, COLS))
        m.acc[HALF * h : HALF * (h + 1)] = both.astype(BF16).reshape(HALF, ROWS, COLS)
        for d in (2, 1, 3, 0):
            a = HALF * h + lax.rem(mine_a + d, HALF)
            to = ((z * (1 - c) + a * c) * 16 + (y * c + a * (1 - c)) * 2 + c, t)

            def reply(a=a, to=to):
                send(m.acc.at[a], m.fin.at[mine_a], m.s_y, m.r_y, to)

            if d:
                reply()
                continue
            own = mine_a // HALF == h

            @pl.when(jnp.logical_not(own))
            def _(reply=reply):
                reply()

            @pl.when(own)
            def _():
                m.fin[mine_a] = m.acc[mine_a]

    def dense_in():
        wait(m.dx, m.r_dx)
        for k in range(2):
            wait(dense[k].at[0], m.loc.at[11 + k])
            wait(dense[k].at[pl.ds(1, NZ - 1)], m.r_dw.at[k])
            weights = dense[k][...].reshape(NZ * DH, COLS)
            m.dpart[k, 0:gathered] = dot_nt(
                m.x[:, :, 0:COLS].reshape(gathered, COLS), weights
            ).astype(BF16)
            m.dpart[k, gathered:] = dot_nt(m.dx[...].reshape(gathered, COLS), weights).astype(BF16)
        for d in (2, 1, 3):
            send(m.dpart.at[:, part(d)], m.dparts.at[NT - d], m.s_drs, m.r_drs, at(dt=d))

    def dense_hide():
        wait(m.dparts.at[pl.ds(1, NT - 1)], m.r_drs)
        pre = m.dpart[0, part(0)].astype(F32)
        up = m.dpart[1, part(0)].astype(F32)
        for d in range(1, NT):
            pre = pre + m.dparts[d, 0].astype(F32)
            up = up + m.dparts[d, 1].astype(F32)
        dhidden = (pre / (1.0 + jnp.exp(-pre)) * up).astype(BF16)
        m.dhid[...] = dhidden
        m.dhids[part(0)] = dhidden
        for d in (2, 1, 3):
            send(m.dhid, m.dhids.at[part(0)], m.s_dag, m.r_dag, at(dt=d))

    def dense_out():
        wait(dense[2].at[0], m.loc.at[13])
        wait(dense[2].at[pl.ds(1, NZ - 1)], m.r_dw.at[2])
        wait(m.dhids.at[pl.ds(0, 2 * gathered - quarter)], m.r_dag)
        m.dacc[...] = (
            dot(m.dhids[...], m.dd[...].reshape(NZ * DH, COLS))
            .astype(BF16)
            .reshape(NC * NY, ROWS, COLS)
        )
        for d in FAR + (0,):
            a = lax.rem(mine_a + d, NY)
            for e in range(NC):
                if d or e:
                    send(
                        m.dacc.at[NY * e + a],
                        m.dfin.at[NY * e + mine_a],
                        m.s_dy,
                        m.r_dy,
                        at(a=d, dc=e),
                    )
        m.dfin[mine_a] = m.dacc[mine_a]

    def finish():
        wait(m.bgate, m.loc.at[14])
        gate = m.bgate[...].astype(F32)
        branch = jnp.zeros((ROWS, 128), F32)
        for j in range(WIDTH // 128):
            branch = branch + m.ffn[:, 128 * j : 128 * j + 128].astype(F32) * gate[j : j + 1]
        branch = jnp.sum(branch, axis=1, keepdims=True)
        branch = 1.0 / (1.0 + jnp.exp(-branch))
        wait(m.dfin.at[pl.ds(1, NC * NY - 1)], m.r_dy)
        total = m.dfin[0].astype(F32)
        for d in range(1, NC * NY):
            total = total + m.dfin[d].astype(F32)
        total = m.after[:, block(0)] + branch * total
        wait(m.fin.at[pl.ds(1, NY - 1)], m.r_y)
        for d in range(NY):
            total = total + m.fin[d].astype(F32)
        out[...] = total.astype(BF16)

    def meet(core, count, sem):
        @pl.when(c == core)
        def _():
            pl.semaphore_wait(barrier, count)
            pl.semaphore_signal(sem, 1, device_id=at(dc=1), device_id_type=MESH)

        @pl.when(c != core)
        def _():
            pl.semaphore_wait(sem, 1)

    meet(0, NC * (NT - 1) + 1, m.near)
    mix()
    meet(1, NC * (NY - 1 + NZ - 1) + 1, m.wide)
    spread_routes()
    spread(0)
    spread(1)
    gather()
    gather_other()
    split_down()
    assign()
    pl.when((c == 1) | (near_half == 0))(lambda: emit(0))
    pl.when((c == 0) & (near_half == 0))(lambda: emit(1))
    pl.when((c == 0) & (near_half == 1))(lambda: emit(0))
    pl.when((c == 1) | (near_half == 1))(lambda: emit(1))
    dense_in()
    up_ready()
    trade(0, 1)
    trade(0, 0)
    trade(1, 1)
    trade(1, 0)
    spread(2)
    hide(0, 1)
    hide(0, 0)
    hide(1, 1)
    hide(1, 0)
    dense_hide()
    down_ready()
    answer(0, 1)
    answer(0, 0)
    answer(1, 1)
    answer(1, 0)
    dense_out()
    pl.when((c == 1) | (near_half == 0))(lambda: combine(0))
    pl.when((c == 0) & (near_half == 0))(lambda: combine(1))
    pl.when((c == 0) & (near_half == 1))(lambda: combine(0))
    pl.when((c == 1) | (near_half == 1))(lambda: combine(1))
    finish()

    wait(m.hp.at[pl.ds(1, NT - 1)], m.s_hp)
    wait(m.rt.at[pl.ds(1, NY - 1)], m.s_rt)
    wait(m.sc.at[pl.ds(1, NY - 1)], m.s_sc)
    wait(m.wdn.at[pl.ds(1, NT - 1)], m.s_wdn)
    wait(m.x.at[pl.ds(1, NY - 1)], m.s_x)
    wait(m.dx, m.s_dx)
    for k in range(3):
        wait(dense[k].at[pl.ds(1, NZ - 1)], m.s_dw.at[k])
    wait(m.slots.at[:, pl.ds(0, NE - 1)], m.s_z)
    wait(m.got.at[:, :, :, right], m.s_up)
    wait(m.hids.at[:, :, pl.ds(HID, (NT - 1) * HID)], m.s_ag)
    wait(m.dparts.at[pl.ds(1, NT - 1)], m.s_drs)
    wait(m.dhids.at[pl.ds(0, 2 * gathered - quarter)], m.s_dag)
    wait(m.back.at[:, pl.ds(0, NE - 1)], m.s_rz)
    wait(m.dfin.at[pl.ds(1, NC * NY - 1)], m.s_dy)
    wait(m.fin.at[pl.ds(1, NY - 1)], m.s_y)


def on_device(
    tokens,
    positions,
    state,
    mix_gain,
    w_query,
    w_key,
    w_value,
    w_out,
    ffn_gain,
    branch_gate,
    dense_gate,
    dense_up,
    dense_down,
    routes,
    route_scores,
    expert_gate,
    expert_up,
    expert_down,
):
    half = HEAD // 2
    inverse = 10000.0 ** -(np.arange(half, dtype=np.float64) / (half - 1))
    freq = jnp.asarray(np.concatenate([inverse, inverse])[None], F32)
    args = (
        tokens,
        positions.reshape(1, ROWS),
        state.reshape(ROWS, HEAD, HEAD),
        mix_gain.reshape(WIDTH // 128, 128),
        w_query,
        w_key,
        w_value,
        w_out,
        ffn_gain.reshape(WIDTH // 128, 128),
        branch_gate.reshape(WIDTH // 128, 128),
        dense_gate.T,
        dense_up.T,
        dense_down,
        routes.T,
        route_scores.T,
        expert_gate.reshape(WIDTH, HID),
        expert_up.reshape(WIDTH, HID),
        expert_down.reshape(HID, WIDTH),
        freq,
    )
    return pl.pallas_call(
        kernel,
        name="layer",
        out_shape=pltpu.VMEM((ROWS, COLS), BF16),
        in_specs=[pl.BlockSpec(memory_space=pltpu.HBM)] * len(args),
        out_specs=pl.BlockSpec(memory_space=pltpu.VMEM),
        scratch_shapes=list(scratch_table().values()),
        compiler_params=pltpu.CompilerParams(
            collective_id=0, has_side_effects=True, vmem_limit_bytes=60 * 1024 * 1024
        ),
    )(*args)


def solution(mesh):
    placed = (
        P("ep", None),
        P("ep"),
        P("ep", "tp", None, None),
        P(),
        P(None, "tp"),
        P(None, "tp"),
        P(None, "tp"),
        P("tp", None),
        P(),
        P(),
        P("tp", "ep"),
        P("tp", "ep"),
        P("ep", "tp"),
        P("ep", None),
        P("ep", None),
        P("ep", None, "tp"),
        P("ep", None, "tp"),
        P("ep", "tp", None),
    )
    return jax.shard_map(
        on_device, mesh=mesh, in_specs=placed, out_specs=P("ep", "tp"), check_vma=False
    )
```

```python
import types

import jax
import jax.numpy as jnp
import numpy as np
from jax import lax
from jax.experimental import pallas as pl
from jax.experimental.pallas import tpu as pltpu
from jax.sharding import PartitionSpec as P

EPS = 1e-06
MESH = pl.DeviceIdType.MESH
F32 = jnp.float32
BF16 = jnp.bfloat16
NZ, NY, NC, NT = 8, 8, 2, 4
ROWS = 16
WIDTH = 2048
HEAD = 128
COLS = WIDTH // NT
HID = 128
DH = 32
NE = NZ * NC
HALF = NZ // 2
WAVES = 2
UNIT = 8
FAR = (4, 3, 5, 2, 6, 1, 7)


def dot(a, b):
    return jnp.dot(a, b, preferred_element_type=F32)


def dot_nt(a, b):
    return lax.dot_general(a, b, (((1,), (1,)), ((), ())), preferred_element_type=F32)


def dot_tn(a, b):
    return lax.dot_general(a, b, (((0,), (0,)), ((), ())), preferred_element_type=F32)


def scratch_table():
    dma = pltpu.SemaphoreType.DMA
    gathered = NY * ROWS
    wave = NE * UNIT
    return dict(
        tok=pltpu.VMEM((ROWS, WIDTH), BF16),
        pos=pltpu.VMEM((1, ROWS), jnp.int32),
        state=pltpu.VMEM((ROWS, HEAD, HEAD), F32),
        mixg=pltpu.VMEM((WIDTH // 128, 128), F32),
        wqkv=pltpu.VMEM((WIDTH, 3 * HEAD), BF16),
        wout=pltpu.VMEM((HEAD, WIDTH), BF16),
        ffng=pltpu.VMEM((WIDTH // 128, 128), F32),
        bgate=pltpu.VMEM((WIDTH // 128, 128), BF16),
        freq=pltpu.VMEM((1, 128), F32),
        hp=pltpu.VMEM((NT, ROWS, WIDTH), BF16),
        after=pltpu.VMEM((ROWS, WIDTH), F32),
        ffn=pltpu.VMEM((ROWS, WIDTH), BF16),
        x=pltpu.VMEM((NY, ROWS, 2 * COLS), BF16),
        rt=pltpu.VMEM((NY, 6, ROWS), jnp.int32),
        sc=pltpu.VMEM((NY, 6, ROWS), F32),
        place=pltpu.VMEM((2, wave, gathered // 2), BF16),
        weigh=pltpu.VMEM((2, wave, gathered // 2), BF16),
        slots=pltpu.VMEM((2, NE, UNIT, 2 * COLS), BF16),
        got=pltpu.VMEM((WAVES, NE, UNIT, WIDTH), BF16),
        wgu=pltpu.VMEM((WIDTH, 2 * HID), BF16),
        wdn=pltpu.VMEM((NT, HID, COLS), BF16),
        half=pltpu.VMEM((WAVES, wave, 2 * HID), F32),
        hid=pltpu.VMEM((WAVES, wave, HID), BF16),
        hids=pltpu.VMEM((WAVES, wave, NT * HID), BF16),
        rows=pltpu.VMEM((WAVES, NE, UNIT, COLS), BF16),
        back=pltpu.VMEM((2, NE, UNIT, COLS), BF16),
        acc=pltpu.VMEM((NY, ROWS, COLS), BF16),
        fin=pltpu.VMEM((NY, ROWS, COLS), BF16),
        dx=pltpu.VMEM((NY, ROWS, COLS), BF16),
        dg=pltpu.VMEM((NZ, DH, COLS), BF16),
        du=pltpu.VMEM((NZ, DH, COLS), BF16),
        dd=pltpu.VMEM((NZ, DH, COLS), BF16),
        dpart=pltpu.VMEM((2, 2 * gathered, NZ * DH), BF16),
        dparts=pltpu.VMEM((NT, 2, 2 * gathered // NT, NZ * DH), BF16),
        dhid=pltpu.VMEM((2 * gathered // NT, NZ * DH), BF16),
        dhids=pltpu.VMEM((2 * gathered, NZ * DH), BF16),
        dacc=pltpu.VMEM((NC * NY, ROWS, COLS), BF16),
        dfin=pltpu.VMEM((NC * NY, ROWS, COLS), BF16),
        near=pltpu.SemaphoreType.REGULAR,
        wide=pltpu.SemaphoreType.REGULAR,
        loc=dma((16,)),
        s_hp=dma,
        r_hp=dma,
        s_wdn=dma,
        r_wdn=dma,
        s_rt=dma,
        r_rt=dma,
        s_sc=dma,
        r_sc=dma,
        s_x=dma,
        r_x=dma((2,)),
        s_dx=dma,
        r_dx=dma,
        s_dw=dma((3,)),
        r_dw=dma((3,)),
        s_z=dma,
        r_z=dma((2 * WAVES,)),
        s_up=dma,
        r_up=dma((2 * WAVES,)),
        s_ag=dma,
        r_ag=dma((2 * WAVES,)),
        s_rz=dma,
        r_rz=dma((2,)),
        s_drs=dma,
        r_drs=dma,
        s_dag=dma,
        r_dag=dma,
        s_dy=dma,
        r_dy=dma,
        s_y=dma,
        r_y=dma,
    )


def kernel(
    tokens,
    positions,
    state,
    mix_gain,
    w_query,
    w_key,
    w_value,
    w_out,
    ffn_gain,
    branch_gate,
    dense_gate,
    dense_up,
    dense_down,
    routes,
    scores,
    expert_gate,
    expert_up,
    expert_down,
    freq,
    out,
    *scratch,
):
    m = types.SimpleNamespace(**dict(zip(scratch_table(), scratch)))
    ep = lax.axis_index("ep")
    t = lax.axis_index("tp")
    z, y, c = ep // 16, (ep // 2) % 8, ep % 2

    def at(a=0, b=0, dc=0, dt=0):
        to_z = lax.rem(z + a * c + b * (1 - c), NZ)
        to_y = lax.rem(y + a * (1 - c) + b * c, NY)
        return (to_z * 16 + to_y * 2 + lax.rem(c + dc, NC), lax.rem(t + dt, NT))

    def send(src, dst, s, r, dev):
        pltpu.make_async_remote_copy(
            src_ref=src, dst_ref=dst, send_sem=s, recv_sem=r, device_id=dev, device_id_type=MESH
        ).start()

    def wait(ref, sem):
        pltpu.make_async_copy(ref, ref, sem).wait()

    def block(d):
        return pl.ds(pl.multiple_of(lax.rem(t + d, NT) * COLS, COLS), COLS)

    near_half = z // HALF
    mine_a = y * (1 - c) + z * c
    mine_b = z * (1 - c) + y * c

    def fetch(k, *pairs):
        for src, dst in pairs:
            pltpu.make_async_copy(src, dst, m.loc.at[k]).start()

    fetch(0, (tokens, m.tok))
    fetch(1, (mix_gain, m.mixg))
    fetch(2, (positions, m.pos))
    fetch(3, (freq, m.freq))
    fetch(
        4,
        *[
            (n, m.wqkv.at[:, pl.ds(HEAD * k, HEAD)])
            for k, n in enumerate((w_query, w_key, w_value))
        ],
    )
    fetch(5, (state, m.state))
    fetch(6, (w_out, m.wout))

    barrier = pltpu.get_barrier_semaphore()

    def greet(dz, dy, dx, core):
        to = lax.rem(z + dz, NZ) * 16 + lax.rem(y + dy, NY) * 2 + core
        pl.semaphore_signal(
            barrier, 1, device_id=(to, lax.rem(t + dx, NT)), device_id_type=MESH
        )

    for d in range(1, NT):
        greet(0, 0, d, 0)
    for d in range(1, NY):
        greet(0, d, 0, 1)
    for d in range(1, NZ):
        greet(d, 0, 0, 1)

    @pl.when(c == 0)
    def _():
        greet(0, 0, 0, 1)

    @pl.when(c == 1)
    def _():
        greet(0, 0, 0, 0)

    wait(m.tok, m.loc.at[0])
    wait(m.mixg, m.loc.at[1])
    tok = m.tok[...].astype(F32)
    scale = lax.rsqrt(jnp.mean(tok * tok, axis=1, keepdims=True) + EPS)
    gain = m.mixg[...]
    normed = jnp.concatenate(
        [
            (tok[:, 128 * j : 128 * j + 128] * scale * gain[j : j + 1]).astype(BF16)
            for j in range(WIDTH // 128)
        ],
        axis=1,
    )
    wait(m.pos, m.loc.at[2])
    wait(m.freq, m.loc.at[3])
    eye = lax.broadcasted_iota(jnp.int32, (ROWS, ROWS), 0) == lax.broadcasted_iota(
        jnp.int32, (ROWS, ROWS), 1
    )
    where = jnp.sum(jnp.where(eye, m.pos[...].astype(F32), 0.0), axis=1, keepdims=True)
    angle = where * m.freq[...]
    lane = lax.broadcasted_iota(jnp.int32, (ROWS, HEAD), 1)
    cosine = jnp.cos(angle)
    sine = jnp.where(lane < HEAD // 2, -jnp.sin(angle), jnp.sin(angle))
    wait(m.wqkv, m.loc.at[4])
    qkv = dot(normed, m.wqkv[...])
    query, key, value = (qkv[:, HEAD * k : HEAD * (k + 1)] for k in range(3))

    def rotate(v):
        return v * cosine + pltpu.roll(v, HEAD // 2, 1) * sine

    query = rotate(query)
    key = rotate(key) * HEAD**-0.5
    head = t.astype(F32)
    decay = 1.0 - jnp.exp2(jnp.full((1, HEAD), -5.0 - 5.0 * head / (NT - 1), F32))
    row = lax.broadcasted_iota(jnp.int32, (ROWS, HEAD), 0)
    apart = jnp.concatenate(
        [jnp.where(row == s, query, 0.0).astype(BF16) for s in range(ROWS)], axis=1
    )
    wait(m.state, m.loc.at[5])
    held = dot(apart, m.state[...].reshape(ROWS * HEAD, HEAD).astype(BF16))
    retrieved = held * decay + jnp.sum(query * key, axis=1, keepdims=True) * value
    retrieved = retrieved * lax.rsqrt(
        jnp.mean(retrieved * retrieved, axis=1, keepdims=True) + EPS
    )
    fetch(7, (ffn_gain, m.ffng))
    fetch(8, (routes, m.rt.at[mine_a]))
    fetch(9, (scores, m.sc.at[mine_a]))
    fetch(10, (expert_down.at[:, block(0)], m.wdn.at[0]))
    for k, (src, dst) in enumerate(((dense_gate, m.dg), (dense_up, m.du), (dense_down, m.dd))):
        fetch(11 + k, (src, dst.at[0]))
    fetch(14, (branch_gate, m.bgate))
    fetch(
        15,
        *[
            (n.at[block(d)], m.wgu.at[pl.ds(COLS * d, COLS), pl.ds(HID * k, HID)])
            for d in range(NT)
            for k, n in enumerate((expert_gate, expert_up))
        ],
    )
    wait(m.wout, m.loc.at[6])
    m.hp[0] = dot(retrieved.astype(BF16), m.wout[...]).astype(BF16)

    gathered = NY * ROWS
    quarter = 2 * gathered // NT
    left = pl.ds(0, 2 * COLS)
    right = pl.ds(2 * COLS, 2 * COLS)
    dense = (m.dg, m.du, m.dd)

    def part(d):
        return pl.ds(pl.multiple_of(lax.rem(t + d, NT) * quarter, quarter), quarter)

    def spread(k):
        src = (dense_gate, dense_up, dense_down)[k]
        for d in FAR:
            send(src, dense[k].at[NZ - d], m.s_dw.at[k], m.r_dw.at[k], at(b=d))

    def spread_routes():
        for d in FAR:
            send(routes, m.rt.at[mine_a], m.s_rt, m.r_rt, at(a=d))
            send(scores, m.sc.at[mine_a], m.s_sc, m.r_sc, at(a=d))

    def split_down():
        for d in (2, 1, 3):
            send(expert_down.at[:, block(d)], m.wdn.at[NT - d], m.s_wdn, m.r_wdn, at(dt=d))

    def mix():
        for d in (2, 1, 3):
            send(m.hp.at[0], m.hp.at[NT - d], m.s_hp, m.r_hp, at(dt=d))

    def gather():
        wait(m.ffng, m.loc.at[7])
        wait(m.hp.at[pl.ds(1, NT - 1)], m.r_hp)
        after = tok
        for d in range(NT):
            after = after + m.hp[d].astype(F32)
        m.after[...] = after
        scale = lax.rsqrt(jnp.mean(after * after, axis=1, keepdims=True) + EPS)
        gain = m.ffng[...]
        for j in range(WIDTH // 128):
            m.ffn[:, 128 * j : 128 * j + 128] = (
                after[:, 128 * j : 128 * j + 128] * scale * gain[j : j + 1]
            ).astype(BF16)
        for d in range(2):
            m.x[mine_a, :, COLS * d : COLS * (d + 1)] = m.ffn[:, block(d)]
        for d in FAR:
            send(m.x.at[mine_a], m.x.at[mine_a], m.s_x, m.r_x.at[mine_a // HALF], at(a=d))

    def gather_other():
        for d in FAR + (0,):
            send(
                m.x.at[mine_a, :, pl.ds(0, COLS)],
                m.dx.at[mine_b],
                m.s_dx,
                m.r_dx,
                at(b=d, dc=1),
            )

    def assign():
        wait(m.rt.at[0], m.loc.at[8])
        wait(m.sc.at[0], m.loc.at[9])
        wait(m.rt.at[pl.ds(1, NY - 1)], m.r_rt)
        wait(m.sc.at[pl.ds(1, NY - 1)], m.r_sc)
        tokens_h = HALF * ROWS
        k = lax.broadcasted_iota(jnp.int32, (NE, tokens_h), 0)
        lane = lax.broadcasted_iota(jnp.int32, (NE, tokens_h), 1)
        expert = ((k // 2) * (1 - c) + z * c) * 16 + ((k // 2) * c + y * (1 - c)) * 2 + (k & 1)
        a = lax.broadcasted_iota(jnp.int32, (tokens_h, tokens_h), 0)
        b = lax.broadcasted_iota(jnp.int32, (tokens_h, tokens_h), 1)
        ahead = jnp.where((a // ROWS == b // ROWS) & (a < b), 1.0, 0.0).astype(BF16)
        slot = lax.broadcasted_iota(jnp.int32, (UNIT, tokens_h), 0).astype(F32)
        for h in range(2):
            some = range(HALF * h, HALF * (h + 1))
            chosen = jnp.concatenate([m.rt[d] for d in some], axis=1)
            scored = jnp.concatenate([m.sc[d] for d in some], axis=1)
            shares = scored / jnp.sum(scored, axis=0, keepdims=True)
            named = jnp.zeros((NE, tokens_h), F32)
            share = jnp.zeros((NE, tokens_h), F32)
            for n in range(6):
                hit = chosen[n : n + 1] == expert
                named = jnp.where(hit, 1.0, named)
                share = jnp.where(hit, shares[n : n + 1], share)
            rank = dot(named.astype(BF16), ahead)
            code = jnp.where(named > 0.5, rank + (2 * (lane // ROWS)).astype(F32), -1.0)
            for n in range(NE):
                hit = code[n : n + 1] == slot
                at_n = pl.ds(UNIT * n, UNIT)
                m.place[h, at_n, :] = jnp.where(hit, 1.0, 0.0).astype(BF16)
                m.weigh[h, at_n, :] = jnp.where(hit, share[n : n + 1], 0.0).astype(BF16)

    def emit(h):
        inside = mine_a // HALF == h

        @pl.when(inside)
        def _():
            wait(m.x.at[pl.ds(0, HALF - 1)], m.r_x.at[h])

        @pl.when(jnp.logical_not(inside))
        def _():
            wait(m.x.at[pl.ds(0, HALF)], m.r_x.at[h])

        m.slots[h] = (
            dot(
                m.place[h],
                m.x[HALF * h : HALF * (h + 1)].reshape(HALF * ROWS, 2 * COLS),
            )
            .astype(BF16)
            .reshape(NE, UNIT, 2 * COLS)
        )
        wave = c * h + (1 - c) * near_half
        for d in (1, 7, 4, 3, 5, 2, 6) + (0,):
            spot = c * (NE // 2 + (NZ - d) % NZ) + (1 - c) * (2 * ((NZ - d) % HALF) + h)
            for e in range(NC):
                k = lax.rem(mine_b + d, NZ) * 2 + lax.rem(c + e, NC)
                if d or e:
                    send(
                        m.slots.at[h, k],
                        m.got.at[wave, spot, :, left],
                        m.s_z,
                        m.r_z.at[2 * wave + c],
                        at(b=d, dc=e),
                    )
                else:
                    m.got[wave, spot, :, left] = m.slots[h, k]

    def up_ready():
        wait(m.wgu, m.loc.at[15])

    def down_ready():
        wait(m.wdn.at[0], m.loc.at[10])
        wait(m.wdn.at[pl.ds(1, NT - 1)], m.r_wdn)

    def trade(w, k):
        n, begin, count = 2 * w + k, NE // 2 * k, NE // 2
        own = (near_half == w) & (c == 0) if k == 0 else c == 1

        @pl.when(own)
        def _():
            wait(m.got.at[w, pl.ds(begin, count - (2 - k)), :, left], m.r_z.at[n])

        @pl.when(jnp.logical_not(own))
        def _():
            wait(m.got.at[w, pl.ds(begin, count), :, left], m.r_z.at[n])

        some = pl.ds(begin, count)
        for j, d in ((0, 1), (1, 3)):
            send(
                m.got.at[w, some, :, pl.ds(COLS * j, COLS)],
                m.got.at[w, some, :, pl.ds(COLS * (3 - j), COLS)],
                m.s_up,
                m.r_up.at[n],
                at(dt=d),
            )
        m.half[w, pl.ds(UNIT * begin, UNIT * count)] = dot(
            m.got[w, begin : begin + count, :, 0 : 2 * COLS].reshape(count * UNIT, 2 * COLS),
            m.wgu[0 : 2 * COLS],
        )

    def hide(w, k):
        n, begin, count = 2 * w + k, NE // 2 * k, NE // 2
        span = pl.ds(UNIT * begin, UNIT * count)
        wait(m.got.at[w, pl.ds(begin, count), :, right], m.r_up.at[n])
        total = m.half[w, span] + dot(
            m.got[w, begin : begin + count, :, 2 * COLS :].reshape(count * UNIT, 2 * COLS),
            m.wgu[2 * COLS :],
        )
        pre = total[:, :HID]
        hidden = (pre / (1.0 + jnp.exp(-pre)) * total[:, HID:]).astype(BF16)
        m.hid[w, span] = hidden
        m.hids[w, span, 0:HID] = hidden
        for d in (2, 1, 3):
            send(
                m.hid.at[w, span],
                m.hids.at[w, span, pl.ds(HID * (NT - d), HID)],
                m.s_ag,
                m.r_ag.at[n],
                at(dt=d),
            )

    def answer(w, k):
        n, begin, count = 2 * w + k, NE // 2 * k, NE // 2
        span = pl.ds(UNIT * begin, UNIT * count)
        wait(m.hids.at[w, span, pl.ds(HID, (NT - 1) * HID)], m.r_ag.at[n])
        m.rows[w, begin : begin + count] = (
            dot(m.hids[w, span], m.wdn[...].reshape(NT * HID, COLS))
            .astype(BF16)
            .reshape(count, UNIT, COLS)
        )

        def reply(spot, to, h, k):
            send(m.rows.at[w, spot], m.back.at[h, k], m.s_rz, m.r_rz.at[h], (to, t))

        for d in (2, 1, 3, 0) if k == 0 else ():
            to = (HALF * w + lax.rem(z + d, HALF)) * 16 + y * 2
            for h in range(2):
                spot, e = 2 * d + h, z * 2 + c
                if d:
                    reply(spot, to, h, e)
                    continue
                own = (c == 0) & (near_half == w)

                @pl.when(jnp.logical_not(own))
                def _(spot=spot, to=to, h=h, e=e):
                    reply(spot, to, h, e)

                @pl.when(own)
                def _(spot=spot, h=h, e=e):
                    m.back[h, e] = m.rows[w, spot]

        for d in FAR + (0,) if k == 1 else ():
            to = z * 16 + lax.rem(y + d, NY) * 2 + 1
            spot, e = NE // 2 + d, y * 2 + c
            if d:
                reply(spot, to, w, e)
                continue

            @pl.when(c == 0)
            def _(spot=spot, to=to, e=e):
                reply(spot, to, w, e)

            @pl.when(c == 1)
            def _(spot=spot, e=e):
                m.back[w, e] = m.rows[w, spot]

    def combine(h):
        wait(m.back.at[h, pl.ds(0, NE - 1)], m.r_rz.at[h])
        both = dot_tn(m.weigh[h], m.back[h].reshape(NE * UNIT, COLS))
        m.acc[HALF * h : HALF * (h + 1)] = both.astype(BF16).reshape(HALF, ROWS, COLS)
        for d in (2, 1, 3, 0):
            a = HALF * h + lax.rem(mine_a + d, HALF)
            to = ((z * (1 - c) + a * c) * 16 + (y * c + a * (1 - c)) * 2 + c, t)

            def reply(a=a, to=to):
                send(m.acc.at[a], m.fin.at[mine_a], m.s_y, m.r_y, to)

            if d:
                reply()
                continue
            own = mine_a // HALF == h

            @pl.when(jnp.logical_not(own))
            def _(reply=reply):
                reply()

            @pl.when(own)
            def _():
                m.fin[mine_a] = m.acc[mine_a]

    def dense_in():
        wait(m.dx, m.r_dx)
        for k in range(2):
            wait(dense[k].at[0], m.loc.at[11 + k])
            wait(dense[k].at[pl.ds(1, NZ - 1)], m.r_dw.at[k])
            weights = dense[k][...].reshape(NZ * DH, COLS)
            m.dpart[k, 0:gathered] = dot_nt(
                m.x[:, :, 0:COLS].reshape(gathered, COLS), weights
            ).astype(BF16)
            m.dpart[k, gathered:] = dot_nt(m.dx[...].reshape(gathered, COLS), weights).astype(BF16)
        for d in (2, 1, 3):
            send(m.dpart.at[:, part(d)], m.dparts.at[NT - d], m.s_drs, m.r_drs, at(dt=d))

    def dense_hide():
        wait(m.dparts.at[pl.ds(1, NT - 1)], m.r_drs)
        pre = m.dpart[0, part(0)].astype(F32)
        up = m.dpart[1, part(0)].astype(F32)
        for d in range(1, NT):
            pre = pre + m.dparts[d, 0].astype(F32)
            up = up + m.dparts[d, 1].astype(F32)
        dhidden = (pre / (1.0 + jnp.exp(-pre)) * up).astype(BF16)
        m.dhid[...] = dhidden
        m.dhids[part(0)] = dhidden
        for d in (2, 1, 3):
            send(m.dhid, m.dhids.at[part(0)], m.s_dag, m.r_dag, at(dt=d))

    def dense_out():
        wait(dense[2].at[0], m.loc.at[13])
        wait(dense[2].at[pl.ds(1, NZ - 1)], m.r_dw.at[2])
        wait(m.dhids.at[pl.ds(0, 2 * gathered - quarter)], m.r_dag)
        m.dacc[...] = (
            dot(m.dhids[...], m.dd[...].reshape(NZ * DH, COLS))
            .astype(BF16)
            .reshape(NC * NY, ROWS, COLS)
        )
        for d in (2, 6, 4, 3, 5, 1, 7) + (0,):
            a = lax.rem(mine_a + d, NY)
            for e in range(NC):
                if d or e:
                    send(
                        m.dacc.at[NY * e + a],
                        m.dfin.at[NY * e + mine_a],
                        m.s_dy,
                        m.r_dy,
                        at(a=d, dc=e),
                    )
        m.dfin[mine_a] = m.dacc[mine_a]

    def finish():
        wait(m.bgate, m.loc.at[14])
        gate = m.bgate[...].astype(F32)
        branch = jnp.zeros((ROWS, 128), F32)
        for j in range(WIDTH // 128):
            branch = branch + m.ffn[:, 128 * j : 128 * j + 128].astype(F32) * gate[j : j + 1]
        branch = jnp.sum(branch, axis=1, keepdims=True)
        branch = 1.0 / (1.0 + jnp.exp(-branch))
        wait(m.dfin.at[pl.ds(1, NC * NY - 1)], m.r_dy)
        total = m.dfin[0].astype(F32)
        for d in range(1, NC * NY):
            total = total + m.dfin[d].astype(F32)
        total = m.after[:, block(0)] + branch * total
        wait(m.fin.at[pl.ds(1, NY - 1)], m.r_y)
        for d in range(NY):
            total = total + m.fin[d].astype(F32)
        out[...] = total.astype(BF16)

    def meet(core, count, sem):
        @pl.when(c == core)
        def _():
            pl.semaphore_wait(barrier, count)
            pl.semaphore_signal(sem, 1, device_id=at(dc=1), device_id_type=MESH)

        @pl.when(c != core)
        def _():
            pl.semaphore_wait(sem, 1)

    meet(0, NC * (NT - 1) + 1, m.near)
    mix()
    meet(1, NC * (NY - 1 + NZ - 1) + 1, m.wide)
    spread_routes()
    spread(0)
    spread(1)
    gather()
    gather_other()
    split_down()
    assign()
    pl.when((c == 1) | (near_half == 0))(lambda: emit(0))
    pl.when((c == 0) & (near_half == 0))(lambda: emit(1))
    pl.when((c == 0) & (near_half == 1))(lambda: emit(0))
    pl.when((c == 1) | (near_half == 1))(lambda: emit(1))
    dense_in()
    up_ready()
    trade(0, 1)
    trade(0, 0)
    trade(1, 1)
    trade(1, 0)
    spread(2)
    hide(0, 1)
    hide(0, 0)
    hide(1, 1)
    hide(1, 0)
    dense_hide()
    down_ready()
    answer(0, 1)
    answer(0, 0)
    answer(1, 1)
    answer(1, 0)
    dense_out()
    pl.when((c == 1) | (near_half == 0))(lambda: combine(0))
    pl.when((c == 0) & (near_half == 0))(lambda: combine(1))
    pl.when((c == 0) & (near_half == 1))(lambda: combine(0))
    pl.when((c == 1) | (near_half == 1))(lambda: combine(1))
    finish()

    wait(m.hp.at[pl.ds(1, NT - 1)], m.s_hp)
    wait(m.rt.at[pl.ds(1, NY - 1)], m.s_rt)
    wait(m.sc.at[pl.ds(1, NY - 1)], m.s_sc)
    wait(m.wdn.at[pl.ds(1, NT - 1)], m.s_wdn)
    wait(m.x.at[pl.ds(1, NY - 1)], m.s_x)
    wait(m.dx, m.s_dx)
    for k in range(3):
        wait(dense[k].at[pl.ds(1, NZ - 1)], m.s_dw.at[k])
    wait(m.slots.at[:, pl.ds(0, NE - 1)], m.s_z)
    wait(m.got.at[:, :, :, right], m.s_up)
    wait(m.hids.at[:, :, pl.ds(HID, (NT - 1) * HID)], m.s_ag)
    wait(m.dparts.at[pl.ds(1, NT - 1)], m.s_drs)
    wait(m.dhids.at[pl.ds(0, 2 * gathered - quarter)], m.s_dag)
    wait(m.back.at[:, pl.ds(0, NE - 1)], m.s_rz)
    wait(m.dfin.at[pl.ds(1, NC * NY - 1)], m.s_dy)
    wait(m.fin.at[pl.ds(1, NY - 1)], m.s_y)


def on_device(
    tokens,
    positions,
    state,
    mix_gain,
    w_query,
    w_key,
    w_value,
    w_out,
    ffn_gain,
    branch_gate,
    dense_gate,
    dense_up,
    dense_down,
    routes,
    route_scores,
    expert_gate,
    expert_up,
    expert_down,
):
    half = HEAD // 2
    inverse = 10000.0 ** -(np.arange(half, dtype=np.float64) / (half - 1))
    freq = jnp.asarray(np.concatenate([inverse, inverse])[None], F32)
    args = (
        tokens,
        positions.reshape(1, ROWS),
        state.reshape(ROWS, HEAD, HEAD),
        mix_gain.reshape(WIDTH // 128, 128),
        w_query,
        w_key,
        w_value,
        w_out,
        ffn_gain.reshape(WIDTH // 128, 128),
        branch_gate.reshape(WIDTH // 128, 128),
        dense_gate.T,
        dense_up.T,
        dense_down,
        routes.T,
        route_scores.T,
        expert_gate.reshape(WIDTH, HID),
        expert_up.reshape(WIDTH, HID),
        expert_down.reshape(HID, WIDTH),
        freq,
    )
    return pl.pallas_call(
        kernel,
        name="layer",
        out_shape=pltpu.VMEM((ROWS, COLS), BF16),
        in_specs=[pl.BlockSpec(memory_space=pltpu.HBM)] * len(args),
        out_specs=pl.BlockSpec(memory_space=pltpu.VMEM),
        scratch_shapes=list(scratch_table().values()),
        compiler_params=pltpu.CompilerParams(
            collective_id=0, has_side_effects=True, vmem_limit_bytes=60 * 1024 * 1024
        ),
    )(*args)


def solution(mesh):
    placed = (
        P("ep", None),
        P("ep"),
        P("ep", "tp", None, None),
        P(),
        P(None, "tp"),
        P(None, "tp"),
        P(None, "tp"),
        P("tp", None),
        P(),
        P(),
        P("tp", "ep"),
        P("tp", "ep"),
        P("ep", "tp"),
        P("ep", None),
        P("ep", None),
        P("ep", None, "tp"),
        P("ep", None, "tp"),
        P("ep", "tp", None),
    )
    return jax.shard_map(
        on_device, mesh=mesh, in_specs=placed, out_specs=P("ep", "tp"), check_vma=False
    )
```
